128 devices in a mesh: sp: 16 (over z, y), tp: 8 (over x, core).
Axes of the slice: x: 4, y: 4, z: 4, core: 2. Of those that a mesh axis runs over, the one named last changes fastest.
Arguments:
- layer_input_rows: bfloat16 [4096, 2048], P('sp'), may hold values from -6 to 6
- input_norm_gain: float32 [2048], replicated, may hold values from 0.1 to 1.9
- query_weight: bfloat16 [2048, 1024], P(None, 'tp'), may hold values from -0.125 to 0.125
- key_weight: bfloat16 [2048, 1024], P(None, 'tp'), may hold values from -0.125 to 0.125
- value_weight: bfloat16 [2048, 1024], P(None, 'tp'), may hold values from -0.125 to 0.125
- query_norm_gain: float32 [64], replicated, may hold values from 0.5 to 9
- key_norm_gain: float32 [64], replicated, may hold values from 0.5 to 9
- cumulative_gate: float32 [4096, 16], P('sp', 'tp'), may hold values from -575.44 to 0, as said below
- attention_norm_gain: float32 [1024], P('tp'), may hold values from 0.1 to 1.9
- recurrence_query_weight: bfloat16 [2048, 1024], P(None, 'tp'), may hold values from -0.125 to 0.125
- forget_weight: bfloat16 [2048, 1024], P(None, 'tp'), may hold values from -0.125 to 0.125
- recurrence_value_weight: bfloat16 [2048, 1024], P(None, 'tp'), may hold values from -0.125 to 0.125
- output_gate_weight: bfloat16 [2048, 1024], P(None, 'tp'), may hold values from -0.125 to 0.125
- gate_lower_slack: float32 [1024], P('tp'), may hold values from 0 to 0.06
- extra_log_decay: float32 [4096, 8], P('sp', 'tp'), may hold values from -1.5 to 0
- recurrence_norm_gain: float32 [1024], P('tp'), may hold values from 0.1 to 1.9
- attention_output_weight: bfloat16 [1024, 2048], P('tp'), may hold values from -0.125 to 0.125
- recurrence_output_weight: bfloat16 [1024, 2048], P('tp'), may hold values from -0.125 to 0.125
Outputs:
- mixed: bfloat16 [4096, 2048], P(('sp', 'tp'))
- log_sum: float32 [4096, 16], P('sp', 'tp')
The draws below stay inside these ranges and needn't reach their ends.
Inputs may be any that keep to these rules, and one draw needn't show every extreme that they name: `cumulative_gate`: each column never rises along positions.
All inputs are finite; a program needn't handle non-finite values.
Results may differ from the reference program's by a relative error of at most 0.015.
The reference program's roundings to bfloat16 on the way count: a program that leaves them out, or rounds other values in their place, can miss the bound.
Values may be sent and summed in bfloat16 or wider, within the bound.
No kernel may reach another device: no remote copies, remote signals or barrier semaphores. Data moves between devices by JAX's collectives and lax.ppermute only.
A program may use at most 64 MiB of HBM per device.

```python
import math
import jax
import jax.numpy as jnp
from jax import lax

D = 2048
ATT_HEADS = 16
HEAD_DIM = 64
RECURRENCE_HEADS = 8
STATE_ROWS = 128
VAL_DIM = 128
BLOCK = 64
TOKEN_COUNT = 4096
N_TP = 8


def gain_draw(base_key, salt_value):
    subkey = jax.random.fold_in(base_key, salt_value)
    return 1.0 + 0.18 * jax.random.truncated_normal(subkey, -2.5, 2.5, (HEAD_DIM,), jnp.float32)


def draw_query_norm_gain(key, part):
    return gain_draw(key, 11)


def draw_key_norm_gain(key, part):
    return gain_draw(key, 12)


def rough_logs(base_key, head_number, rates):
    random_subkeys = jax.random.split(base_key, 4)
    position_index = jnp.arange(TOKEN_COUNT, dtype=jnp.int32)
    block_of = position_index * 32 // TOKEN_COUNT
    factors = jnp.exp(jax.random.uniform(random_subkeys[0], (32, head_number), jnp.float32, -0.7, 0.7))
    block_scale = jnp.take(factors, block_of, axis=0)
    roughness = jax.random.uniform(random_subkeys[1], (TOKEN_COUNT, head_number), jnp.float32, 0.0, 2.0)
    logit_values = -rates[None, :] * block_scale * roughness
    spike_position = jax.random.randint(random_subkeys[2], (2, head_number), 0, TOKEN_COUNT)
    spike_depth = jnp.log(jax.random.uniform(random_subkeys[3], (2, head_number), jnp.float32, 0.5, 0.8))
    spike_hits = (position_index[:, None, None] == spike_position[None]).astype(jnp.float32)
    return logit_values + jnp.sum(spike_hits * spike_depth[None], axis=1)


def draw_cumulative_gate(key, part):
    random_subkeys = jax.random.split(jax.random.fold_in(key, 21), 4)
    ranking = jax.random.permutation(random_subkeys[0], ATT_HEADS)
    fast_count = ATT_HEADS // 2
    slow_heads = ranking >= fast_count
    slow_rate = jnp.exp(jax.random.uniform(random_subkeys[1], (ATT_HEADS,), jnp.float32, -0.69, 0.69)) / TOKEN_COUNT
    fast_rate = jnp.exp(jax.random.uniform(random_subkeys[2], (ATT_HEADS,), jnp.float32, -4.6, -3.4))
    rates = jnp.where(slow_heads, slow_rate, fast_rate)
    return jnp.cumsum(rough_logs(random_subkeys[3], ATT_HEADS, rates), axis=0)


def draw_extra_log_decay(key, part):
    random_subkeys = jax.random.split(jax.random.fold_in(key, 31), 2)
    rates = jnp.exp(jax.random.uniform(random_subkeys[0], (RECURRENCE_HEADS,), jnp.float32, -2.3, -0.22)) / TOKEN_COUNT
    return rough_logs(random_subkeys[1], RECURRENCE_HEADS, rates)


def draw_gate_lower_slack(key, part):
    random_subkeys = jax.random.split(jax.random.fold_in(key, 41), 3)
    channels = RECURRENCE_HEADS * STATE_ROWS
    ranking = jax.random.permutation(random_subkeys[0], channels)
    fast_count = channels // 2
    slow_rows = ranking >= fast_count
    slow_gap = jnp.exp(jax.random.uniform(random_subkeys[1], (channels,), jnp.float32, -1.6, 0.0)) / TOKEN_COUNT
    fast_gap = jnp.exp(jax.random.uniform(random_subkeys[2], (channels,), jnp.float32, -3.9, -2.82))
    return jnp.where(slow_rows, slow_gap, fast_gap)


def steps_of(rng, shape, cuts, smallest, high):
    loudness = 1.0
    for axis_at, parts in cuts:
        steps = jax.random.uniform(jax.random.fold_in(jax.random.fold_in(rng, 6), axis_at), (parts,), jnp.float32, smallest / len(cuts), high / len(cuts))
        loudness = loudness * jnp.repeat(jnp.exp(steps), shape[axis_at] // parts).reshape((-1,) + (1,) * (len(shape) - 1 - axis_at))
    return loudness


def centred(own_key, extent, spread, limit, pieces=(), kind=jnp.bfloat16):
    level = steps_of(own_key, extent, pieces, -0.22, 0.18) if pieces else 1.0
    array = jax.random.normal(own_key, extent, jnp.float32) * spread * level
    return jnp.minimum(jnp.maximum(array, -limit), limit).astype(kind)


def setup_inputs(seed: int = 0) -> dict:
    arg_keys = jax.random.split(jax.random.key(seed), 19)
    return {
        "layer_input_rows": centred(arg_keys[0], (TOKEN_COUNT, D), 1.0, 6.0, ((0, 16),)),
        "input_norm_gain": jnp.clip(1.0 + 0.18 * jax.random.normal(arg_keys[1], (D,), jnp.float32), 0.1, 1.9),
        "query_weight": centred(arg_keys[2], (D, ATT_HEADS * HEAD_DIM), D ** -0.5, 0.125, ((1, 8),)),
        "key_weight": centred(arg_keys[3], (D, ATT_HEADS * HEAD_DIM), D ** -0.5, 0.125, ((1, 8),)),
        "value_weight": centred(arg_keys[4], (D, ATT_HEADS * HEAD_DIM), D ** -0.5, 0.125, ((1, 8),)),
        "query_norm_gain": draw_query_norm_gain(jax.random.fold_in(arg_keys[18], 71), 0),
        "key_norm_gain": draw_key_norm_gain(jax.random.fold_in(arg_keys[18], 71), 0),
        "cumulative_gate": draw_cumulative_gate(jax.random.fold_in(arg_keys[18], 71), 0),
        "attention_norm_gain": jnp.clip(1.0 + 0.18 * jax.random.normal(arg_keys[8], (ATT_HEADS * HEAD_DIM,), jnp.float32), 0.1, 1.9),
        "recurrence_query_weight": centred(arg_keys[9], (D, RECURRENCE_HEADS * STATE_ROWS), D ** -0.5, 0.125, ((1, 8),)),
        "forget_weight": centred(arg_keys[10], (D, RECURRENCE_HEADS * STATE_ROWS), D ** -0.5, 0.125, ((1, 8),)),
        "recurrence_value_weight": centred(arg_keys[11], (D, RECURRENCE_HEADS * VAL_DIM), D ** -0.5, 0.125, ((1, 8),)),
        "output_gate_weight": centred(arg_keys[12], (D, RECURRENCE_HEADS * VAL_DIM), D ** -0.5, 0.125, ((1, 8),)),
        "gate_lower_slack": draw_gate_lower_slack(jax.random.fold_in(arg_keys[18], 71), 0),
        "extra_log_decay": draw_extra_log_decay(jax.random.fold_in(arg_keys[18], 71), 0),
        "recurrence_norm_gain": jnp.clip(1.0 + 0.18 * jax.random.normal(arg_keys[15], (RECURRENCE_HEADS * VAL_DIM,), jnp.float32), 0.1, 1.9),
        "attention_output_weight": centred(arg_keys[16], (ATT_HEADS * HEAD_DIM, D), (ATT_HEADS * HEAD_DIM + RECURRENCE_HEADS * VAL_DIM) ** -0.5, 0.125, ((0, 8),)),
        "recurrence_output_weight": centred(arg_keys[17], (RECURRENCE_HEADS * VAL_DIM, D), (ATT_HEADS * HEAD_DIM + RECURRENCE_HEADS * VAL_DIM) ** -0.5, 0.125, ((0, 8),)),
    }


EPSILON = 1e-06
HIGHEST_ACCURACY = lax.Precision.HIGHEST

def rms_rows(values, gain):
    squares = lax.optimization_barrier(jnp.mean(values * values, axis=-1, keepdims=True))
    return values * lax.rsqrt(squares + EPSILON) * gain

def recur_blocks(rec_query, forget_fraction, rec_value, decay_logarithm, states):
    length, head_number, keydim = rec_query.shape
    span_rows = BLOCK
    blocks = length // span_rows
    lower_tri = jnp.arange(span_rows)[:, None] >= jnp.arange(span_rows)[None, :]

    def to_blocks(values):
        return values.reshape(blocks, span_rows, head_number, values.shape[-1])

    def advance(carried, inputs):
        current_states, running = carried
        query_block, share_block, value_block, decay_blk = inputs
        within_block = jnp.cumsum(decay_blk, axis=0)
        differ = within_block[:, None] - within_block[None, :]
        fading = jnp.exp(jnp.where(lower_tri[:, :, None, None], differ, -jnp.inf))
        scores = jnp.einsum('thk,tshk,shk->tsh', query_block, fading, share_block, precision=HIGHEST_ACCURACY)
        inner_part = jnp.einsum('tsh,shv->thv', scores, value_block, precision=HIGHEST_ACCURACY)
        carried_piece = jnp.einsum('zbf,bfw->zbw', query_block * jnp.exp(within_block), current_states, precision=HIGHEST_ACCURACY)
        closing_state = within_block[-1]
        current_states = jnp.exp(closing_state)[:, :, None] * current_states + jnp.einsum('tfo,tfw->fow', share_block * jnp.exp(closing_state[None] - within_block), value_block, precision=HIGHEST_ACCURACY)
        visible_query = query_block * jnp.exp(running[None] + within_block)
        return ((current_states, running + closing_state), (inner_part + carried_piece, visible_query))
    zeros_run = jnp.zeros((head_number, keydim), jnp.float32)
    (states, running), (outputs, visible_query) = lax.scan(advance, (states, zeros_run), (to_blocks(rec_query), to_blocks(forget_fraction), to_blocks(rec_value), to_blocks(decay_logarithm)))
    return (outputs.reshape(length, head_number, -1), states, running, visible_query.reshape(length, head_number, keydim))

def attend_head(operands):
    head_query, head_key, head_value, head_cum = operands
    rows_blk = math.gcd(TOKEN_COUNT, 1024)
    score_scale = HEAD_DIM ** (-0.5)
    key_pos = jnp.arange(TOKEN_COUNT, dtype=jnp.int32)

    def one_block(block_index):
        first_row = (block_index * rows_blk).astype(jnp.int32)
        query_block = lax.dynamic_slice_in_dim(head_query, first_row, rows_blk, 0)
        cum_blk = lax.dynamic_slice_in_dim(head_cum, first_row, rows_blk, 0)
        scores = jnp.dot(query_block, head_key.T, preferred_element_type=jnp.float32) * score_scale
        scores = scores + cum_blk[:, None] - head_cum[None, :]
        query_pos = first_row + jnp.arange(rows_blk, dtype=jnp.int32)
        causal = key_pos[None, :] <= query_pos[:, None]
        scores = jnp.where(causal, scores, -jnp.inf)
        row_top = lax.optimization_barrier(jnp.max(scores, axis=-1))
        weights = jnp.exp(scores - row_top[:, None])
        totals = lax.optimization_barrier(jnp.sum(weights, axis=-1))
        summed = jnp.dot(weights.astype(jnp.bfloat16), head_value, preferred_element_type=jnp.float32)
        return (summed / totals[:, None], row_top + jnp.log(totals))
    outputs, log_sums = lax.map(one_block, jnp.arange(TOKEN_COUNT // rows_blk, dtype=jnp.int32))
    return (outputs.reshape(TOKEN_COUNT, HEAD_DIM), log_sums.reshape(TOKEN_COUNT))

def reference(layer_input_rows, input_norm_gain, query_weight, key_weight, value_weight, query_norm_gain, key_norm_gain, cumulative_gate, attention_norm_gain, recurrence_query_weight, forget_weight, recurrence_value_weight, output_gate_weight, gate_lower_slack, extra_log_decay, recurrence_norm_gain, attention_output_weight, recurrence_output_weight):
    normalized_input = rms_rows(layer_input_rows.astype(jnp.float32), input_norm_gain).astype(jnp.bfloat16)

    def project(weight):
        return jnp.dot(normalized_input, weight, preferred_element_type=jnp.float32)
    queries = rms_rows(project(query_weight).reshape(TOKEN_COUNT, ATT_HEADS, HEAD_DIM), query_norm_gain).astype(jnp.bfloat16)
    keys = rms_rows(project(key_weight).reshape(TOKEN_COUNT, ATT_HEADS, HEAD_DIM), key_norm_gain).astype(jnp.bfloat16)
    values = project(value_weight).astype(jnp.bfloat16).reshape(TOKEN_COUNT, ATT_HEADS, HEAD_DIM)
    attention, log_sum = lax.map(attend_head, (queries.transpose(1, 0, 2), keys.transpose(1, 0, 2), values.transpose(1, 0, 2), cumulative_gate.T))
    attn_out = rms_rows(attention.transpose(1, 0, 2), attention_norm_gain.reshape(ATT_HEADS, HEAD_DIM))
    attn_out = attn_out.astype(jnp.bfloat16).reshape(TOKEN_COUNT, ATT_HEADS * HEAD_DIM)
    rec_query = jax.nn.silu(project(recurrence_query_weight)).reshape(TOKEN_COUNT, RECURRENCE_HEADS, STATE_ROWS)
    forget_fraction = gate_lower_slack * jax.nn.sigmoid(-project(forget_weight))
    decay_logarithm = jnp.log1p(-forget_fraction).reshape(TOKEN_COUNT, RECURRENCE_HEADS, STATE_ROWS) + extra_log_decay[:, :, None]
    rec_value = lax.optimization_barrier(project(recurrence_value_weight).astype(jnp.bfloat16)).astype(jnp.float32)
    rec_value = rec_value.reshape(TOKEN_COUNT, RECURRENCE_HEADS, VAL_DIM)
    start_states = jnp.zeros((RECURRENCE_HEADS, STATE_ROWS, VAL_DIM), jnp.float32)
    recurrent_output = recur_blocks(rec_query, forget_fraction.reshape(TOKEN_COUNT, RECURRENCE_HEADS, STATE_ROWS), rec_value, decay_logarithm, start_states)[0]
    out_gate = jax.nn.silu(project(output_gate_weight)).reshape(TOKEN_COUNT, RECURRENCE_HEADS, VAL_DIM)
    rec_out = rms_rows(recurrent_output, recurrence_norm_gain.reshape(RECURRENCE_HEADS, VAL_DIM)) * out_gate
    rec_out = rec_out.astype(jnp.bfloat16).reshape(TOKEN_COUNT, RECURRENCE_HEADS * VAL_DIM)
    attn_cols = ATT_HEADS * HEAD_DIM // N_TP
    rec_cols = RECURRENCE_HEADS * VAL_DIM // N_TP

    def add_group(group_index, running_sum):
        first_attn = (group_index * attn_cols).astype(jnp.int32)
        first_rec = (group_index * rec_cols).astype(jnp.int32)
        attn_part = lax.dynamic_slice_in_dim(attn_out, first_attn, attn_cols, 1)
        attn_rows = lax.dynamic_slice_in_dim(attention_output_weight, first_attn, attn_cols, 0)
        rec_part = lax.dynamic_slice_in_dim(rec_out, first_rec, rec_cols, 1)
        rec_rows = lax.dynamic_slice_in_dim(recurrence_output_weight, first_rec, rec_cols, 0)
        partial_value = jnp.dot(attn_part, attn_rows, preferred_element_type=jnp.float32)
        partial_value = partial_value + jnp.dot(rec_part, rec_rows, preferred_element_type=jnp.float32)
        return running_sum + lax.optimization_barrier(partial_value.astype(jnp.bfloat16)).astype(jnp.float32)
    mixed_sum = lax.fori_loop(0, N_TP, add_group, jnp.zeros((TOKEN_COUNT, D), jnp.float32))
    return (mixed_sum.astype(jnp.bfloat16), log_sum.T)
```

```python
import jax
import jax.numpy as jnp
from jax import lax
from jax.experimental import pallas as pl
from jax.experimental.pallas import tpu as pltpu
from jax.sharding import Mesh
from jax.sharding import PartitionSpec as P

HEAD_DIM = 64
EPSILON = 1e-06
ROWS = 256
WIDE = 2048
F32 = jnp.float32
BF16 = jnp.bfloat16
NEG = -1e30
SP = ("z", "y")
TP = ("x", "c")
MISC = 16
K_AT, V_AT, S_AT, M_AT, Y_ROWS = 0, 256, 512, 640, 656
O_S_AT, O_M_AT, Z_ROWS = 256, 384, 400


def dot(a, b, ca=1, cb=0):
    return lax.dot_general(a, b, (((ca,), (cb,)), ((), ())), preferred_element_type=F32)


def lanes(shape):
    return lax.broadcasted_iota(jnp.int32, shape, len(shape) - 1)


def subs(shape):
    return lax.broadcasted_iota(jnp.int32, shape, 0)


def split3(value):
    high = value.astype(BF16)
    rest = value - high.astype(F32)
    middle = rest.astype(BF16)
    low = (rest - middle.astype(F32)).astype(BF16)
    return high, middle, low


def rows_of(value):
    at_lane, at_row = lanes((MISC, 128)), subs((MISC, 128))
    out = None
    for k, part in enumerate(split3(value)):
        pick = ((at_row == k) & (at_lane == 0)) | ((at_row == 3 + k) & (at_lane == 64))
        piece = dot(jnp.where(pick, 1.0, 0.0).astype(BF16), part, 1, 1)
        out = piece if out is None else out + piece
    return out


def packed_rows(rows, extra_high, extra_low):
    first, second = rows[0:8, 0:128], rows[0:8, 128:256]
    at = subs((8, 128))
    first = jnp.where(at == 6, extra_high, jnp.where(at == 7, extra_low, first))
    return jnp.concatenate([first, second], axis=0).astype(BF16)


def spread_rows(misc):
    at_lane, at_row = lanes((MISC, 128)), subs((MISC, 128))
    halves = []
    for base in (0, 8):
        first = (at_row >= base) & (at_row < base + 3) & (at_lane < 64)
        second = (at_row >= base + 3) & (at_row < base + 6) & (at_lane >= 64)
        halves.append(dot(misc, jnp.where(first | second, 1.0, 0.0).astype(BF16), 0, 0))
    return jnp.concatenate(halves, axis=0)


def pair_of(misc):
    return misc[6:7, :].astype(F32) + misc[7:8, :].astype(F32)


def head_norm(value):
    first = lanes(value.shape) < HEAD_DIM
    squares = value * value
    one = jnp.sum(jnp.where(first, squares, 0.0), axis=-1, keepdims=True) / HEAD_DIM
    two = jnp.sum(jnp.where(first, 0.0, squares), axis=-1, keepdims=True) / HEAD_DIM
    return value * jnp.where(first, lax.rsqrt(one + EPSILON), lax.rsqrt(two + EPSILON))


def silu(value):
    return value / (1.0 + jnp.exp(-value))


def project_kernel(
    x_hbm, gain_ref, wq_h, wk_h, wv_h, wrq_h, wf_h, wrv_h, wog_h,
    qg_ref, kg_ref, cum_ref, slack_ref, extra_ref,
    q_ref, msg_ref, inner_ref, vis_ref, og_ref,
    x_v, wk_v, wv_v, wq_v, wf_v, wrq_v, wrv_v, wog_v, sems,
):
    moves = []
    for k, (src, dst) in enumerate(
        [(x_hbm, x_v), (wk_h, wk_v), (wv_h, wv_v), (wq_h, wq_v), (wf_h, wf_v),
         (wrq_h, wrq_v), (wrv_h, wrv_v), (wog_h, wog_v)]
    ):
        move = pltpu.make_async_copy(src, dst, sems.at[k])
        move.start()
        moves.append(move)
    moves[0].wait()
    x = x_v[...].astype(F32)
    mean = jnp.sum(x * x, axis=-1, keepdims=True) / WIDE
    normed = (x * lax.rsqrt(mean + EPSILON) * gain_ref[...]).astype(BF16)

    moves[1].wait()
    moves[2].wait()
    kv = dot(normed, jnp.concatenate([wk_v[...], wv_v[...]], axis=1))
    kgain = jnp.concatenate([kg_ref[...], kg_ref[...]], axis=1)
    qgain = jnp.concatenate([qg_ref[...], qg_ref[...]], axis=1)
    msg_ref[K_AT:V_AT, :] = (head_norm(kv[:, 0:128]) * kgain).astype(BF16)
    msg_ref[V_AT:S_AT, :] = kv[:, 128:256].astype(BF16)

    moves[3].wait()
    moves[4].wait()
    qf = dot(normed, jnp.concatenate([wq_v[...], wf_v[...]], axis=1))
    query = (head_norm(qf[:, 0:128]) * qgain).astype(BF16)
    q_ref[...] = query * jnp.asarray(HEAD_DIM**-0.5, BF16)
    share = slack_ref[...] / (1.0 + jnp.exp(qf[:, 128:256]))
    log_keep = jnp.log1p(-share)

    moves[5].wait()
    moves[6].wait()
    rr = dot(normed, jnp.concatenate([wrq_v[...], wrv_v[...]], axis=1))
    rec_query = silu(rr[:, 0:128])
    rec_value = rr[:, 128:256].astype(BF16)
    moves[7].wait()
    og_ref[...] = silu(dot(normed, wog_v[...]))

    lower = subs((ROWS, ROWS)) >= lanes((ROWS, ROWS))
    tri = jnp.where(lower, 1.0, 0.0).astype(BF16)
    extra = jnp.broadcast_to(extra_ref[...], (ROWS, 128))
    total = None
    for a, b in zip(split3(log_keep), split3(extra)):
        piece = dot(tri, jnp.concatenate([a, b], axis=1))
        total = piece if total is None else total + piece
    own_run, head_run = total[:, 0:128], total[:, 128:256]
    head_rows = rows_of(head_run)
    head_row = head_rows[0:1, :] + head_rows[1:2, :] + head_rows[2:3, :]
    head_col = jnp.concatenate([head_run, head_run], axis=1)
    fading = jnp.exp(jnp.where(lower, head_col - head_row, NEG))
    left = (rec_query * jnp.exp(own_run)).astype(BF16)
    right = (share * jnp.exp(-own_run)).astype(BF16)
    scores = (dot(left, right, 1, 1) * fading).astype(BF16)
    inner_ref[...] = dot(scores, rec_value)
    run = own_run + head_run
    closing = run[ROWS - 1 : ROWS, :]
    vis_ref[...] = (rec_query * jnp.exp(run)).astype(BF16)
    into = (share * jnp.exp(closing - run)).astype(BF16)
    msg_ref[S_AT:M_AT, :] = dot(rec_value, into, 0, 0).astype(BF16)
    first = lanes((ROWS, 128)) < HEAD_DIM
    cum = jnp.where(first, -cum_ref[:, 0:1], -cum_ref[:, 1:2])
    high, middle, _ = split3(closing)
    msg_ref[M_AT:Y_ROWS, :] = packed_rows(rows_of(cum), high.astype(F32), middle.astype(F32))


def key_bias(misc, head):
    misc = misc.astype(F32)
    halves = []
    for base in (0, 8):
        at = base + 3 * head
        halves.append(misc[at : at + 1, :] + misc[at + 1 : at + 2, :] + misc[at + 2 : at + 3, :])
    return jnp.concatenate(halves, axis=1)


def attend(query, msgs, masks):
    keys = jnp.concatenate([m[K_AT:V_AT, :] for m in msgs], axis=0)
    values = jnp.concatenate([m[V_AT:S_AT, :] for m in msgs], axis=0)
    values = jnp.concatenate([values, jnp.ones_like(values)], axis=1)
    first = lanes((ROWS, 128)) < HEAD_DIM
    results = []
    for head in (0, 1):
        mine = jnp.where(first if head == 0 else ~first, query, jnp.zeros_like(query))
        bias = jnp.concatenate([key_bias(m[M_AT:Y_ROWS, :], head) for m in msgs], axis=1)
        scores = dot(mine, keys, 1, 1) + bias
        if masks is not None:
            scores = jnp.where(masks, scores, NEG)
        top = jnp.max(scores, axis=-1, keepdims=True)
        weights = jnp.exp(scores - top).astype(BF16)
        summed = dot(weights, values)
        totals = summed[:, 128:256]
        results.append((summed[:, 0:128] / totals, top + jnp.log(totals)))
    return (
        jnp.where(first, results[0][0], results[1][0]),
        jnp.where(first, results[0][1], results[1][1]),
    )


def places(y):
    return [lax.rem(y - o + 4, 4) for o in range(4)]


def remote_kernel(at_ref, m0, m1, m2, m3, q1, q2, q3, o1, o2, o3):
    z, y = at_ref[0], at_ref[1]
    msgs = (m0, m1, m2, m3)
    where = places(y)
    decays = [pair_of(m[M_AT:Y_ROWS, :]) for m in msgs]
    state = jnp.zeros((128, 128), F32)
    for a in range(4):
        after = jnp.zeros((1, 128), F32)
        for b in range(4):
            if b != a:
                after = after + jnp.where(where[b] > where[a], decays[b], 0.0)
        state = state + msgs[a][S_AT:M_AT, :].astype(F32) * jnp.exp(after)
    state = state.astype(BF16)
    high, middle, _ = split3(decays[0] + decays[1] + decays[2] + decays[3])
    for o, (query, out) in enumerate(((q1, o1), (q2, o2), (q3, o3)), 1):

        @pl.when(z + o < 4)
        def _(query=query, out=out):
            result, log_total = attend(query[...], msgs, None)
            out[0:O_S_AT, :] = result.astype(BF16)
            out[O_S_AT:O_M_AT, :] = state
            out[O_M_AT:Z_ROWS, :] = packed_rows(
                rows_of(log_total), high.astype(F32), middle.astype(F32)
            )


def local_kernel(at_ref, q_ref, m0, m1, m2, m3, inner_ref, vis_ref, o_ref, lse_ref, rec_ref, before_ref):
    y = at_ref[1]
    msgs = (m0, m1, m2, m3)
    where = places(y)
    decays = [pair_of(m[M_AT:Y_ROWS, :]) for m in msgs]
    state = jnp.zeros((128, 128), F32)
    whole = jnp.zeros((1, 128), F32)
    for a in range(1, 4):
        between = jnp.zeros((1, 128), F32)
        for b in range(1, 4):
            if b != a:
                seen = (where[b] > where[a]) & (where[b] < y)
                between = between + jnp.where(seen, decays[b], 0.0)
        piece = msgs[a][S_AT:M_AT, :].astype(F32) * jnp.exp(between)
        state = state + jnp.where(where[a] < y, piece, 0.0)
        whole = whole + jnp.where(where[a] < y, decays[a], 0.0)
    before_ref[...] = jnp.broadcast_to(jnp.exp(whole), (8, 128))
    rec_ref[...] = inner_ref[...] + dot(vis_ref[...], state.astype(BF16), 1, 1)
    shape = (ROWS, 4 * ROWS)
    at = lanes(shape)
    earlier = subs(shape) >= at
    full = jnp.where(y >= 1, 512, 256)
    full = jnp.where(y >= 2, 768, full)
    full = jnp.where(y >= 3, 1024, full)
    masks = earlier | ((at >= 256) & (at < full))
    result, log_total = attend(q_ref[...], msgs, masks)
    o_ref[...] = result
    lse_ref[...] = log_total


def join_kernel(
    at_ref, o_ref, lse_ref, rec_ref, before_ref, vis_ref, og_ref, cum_ref, again_ref, rgain_ref, r1, r2, r3,
    keep_ref, give_ref, log_ref, both_ref,
):
    z, c = at_ref[0], at_ref[2]
    got = (r1, r2, r3)
    lses = [lse_ref[...]]
    outs = [o_ref[...]]
    for o, r in enumerate(got, 1):
        lses.append(jnp.where(z >= o, spread_rows(r[O_M_AT:Z_ROWS, :]), NEG))
        outs.append(r[0:O_S_AT, :].astype(F32))
    top = jnp.maximum(jnp.maximum(lses[0], lses[1]), jnp.maximum(lses[2], lses[3]))
    total, summed = 0.0, 0.0
    for value, out in zip(lses, outs):
        weight = jnp.exp(value - top)
        total = total + weight
        summed = summed + weight * out
    log_total = top + jnp.log(total)
    log_ref[:, 0:1] = log_total[:, 0:1] + cum_ref[:, 0:1]
    log_ref[:, 1:2] = log_total[:, 64:65] + cum_ref[:, 1:2]
    both_ref[:, 0:128] = (head_norm(summed / total) * again_ref[...]).astype(BF16)

    decays = [pair_of(r[O_M_AT:Z_ROWS, :]) for r in got]
    state = r1[O_S_AT:O_M_AT, :].astype(F32)
    state = state + r2[O_S_AT:O_M_AT, :].astype(F32) * jnp.exp(decays[0])
    state = state + r3[O_S_AT:O_M_AT, :].astype(F32) * jnp.exp(decays[0] + decays[1])
    state = (state * before_ref[0:1, :]).astype(BF16)
    rec = rec_ref[...] + dot(vis_ref[...], state, 1, 1)
    mean = jnp.sum(rec * rec, axis=-1, keepdims=True) / 128
    rec = rec * lax.rsqrt(mean + EPSILON) * rgain_ref[...] * og_ref[...]
    both_ref[:, 128:256] = rec.astype(BF16)
    for k in range(4):
        keep_ref[32 * k : 32 * k + 32, :] = both_ref[pl.ds(64 * k + 32 * c, 32), :]
        give_ref[32 * k : 32 * k + 32, :] = both_ref[pl.ds(64 * k + 32 * (1 - c), 32), :]


def out_kernel(at_ref, keep_ref, got_ref, wa, wr, pa, pr, s0, s1, s2, s3, sum_ref):
    x = at_ref[3]
    both = jnp.concatenate([keep_ref[...], got_ref[...]], axis=1)
    for k in range(4):
        cols = slice(512 * k, 512 * k + 512)
        weight = jnp.concatenate([wa[:, cols], wr[:, cols], pa[:, cols], pr[:, cols]], axis=0)
        sum_ref[:, cols] = dot(both, weight).astype(BF16)
    for o, out in enumerate((s0, s1, s2, s3)):
        out[...] = sum_ref[pl.ds(32 * lax.rem(x + o, 4), 32), :]


def add_kernel(a, b, c, d, out):
    out[...] = (
        (a[...].astype(F32) + b[...].astype(F32)) + (c[...].astype(F32) + d[...].astype(F32))
    ).astype(BF16)


VM = pl.BlockSpec(memory_space=pltpu.VMEM)
SM = pl.BlockSpec(memory_space=pltpu.SMEM)
ANY = pl.BlockSpec(memory_space=pl.ANY)


def call(kernel, specs, shapes, scratch=(), name=None):
    return pl.pallas_call(
        kernel,
        in_specs=specs,
        out_specs=[VM] * len(shapes),
        out_shape=[jax.ShapeDtypeStruct(s, d) for s, d in shapes],
        scratch_shapes=list(scratch),
        compiler_params=pltpu.CompilerParams(vmem_limit_bytes=32 * 1024 * 1024),
        name=name,
    )


def turned(value, axis, by):
    return lax.ppermute(value, axis, [(i, (i + by) % 4) for i in range(4)])


def moved(value, axis, by):
    return lax.ppermute(value, axis, [(i, i + by) for i in range(4) if 0 <= i + by < 4])


def body(
    layer_input_rows, input_norm_gain, query_weight, key_weight, value_weight, query_norm_gain,
    key_norm_gain, cumulative_gate, attention_norm_gain, recurrence_query_weight, forget_weight,
    recurrence_value_weight, output_gate_weight, gate_lower_slack, extra_log_decay,
    recurrence_norm_gain, attention_output_weight, recurrence_output_weight,
):
    z, y, x, c = (lax.axis_index(a) for a in ("z", "y", "x", "c"))
    at = jnp.stack([z, y, c, x]).astype(jnp.int32)
    swap = [(0, 1), (1, 0)]
    pa = lax.ppermute(attention_output_weight, "c", swap)
    pr = lax.ppermute(recurrence_output_weight, "c", swap)
    w = pltpu.VMEM((WIDE, 128), BF16)
    tall = (ROWS, 128)
    query, msg, inner, vis, gate = call(
        project_kernel,
        [ANY, VM] + [ANY] * 7 + [VM] * 5,
        [(tall, BF16), ((Y_ROWS, 128), BF16), (tall, F32), (tall, BF16), (tall, F32)],
        [pltpu.VMEM((ROWS, WIDE), BF16)] + [w] * 7 + [pltpu.SemaphoreType.DMA((8,))],
        name="project",
    )(
        layer_input_rows, input_norm_gain.reshape(1, WIDE), query_weight, key_weight, value_weight,
        recurrence_query_weight, forget_weight, recurrence_value_weight, output_gate_weight,
        query_norm_gain.reshape(1, 64), key_norm_gain.reshape(1, 64), cumulative_gate,
        gate_lower_slack.reshape(1, 128), extra_log_decay,
    )
    msgs = [msg] + [turned(msg, "y", o) for o in (1, 2, 3)]
    queries = [moved(query, "z", -o) for o in (1, 2, 3)]
    sent = call(
        remote_kernel, [SM] + [VM] * 7, [((Z_ROWS, 128), BF16)] * 3, name="remote"
    )(at, *msgs, *queries)
    got = [moved(s, "z", o) for o, s in enumerate(sent, 1)]
    out, lse, rec, before = call(
        local_kernel,
        [SM] + [VM] * 7,
        [(tall, F32), (tall, F32), (tall, F32), ((8, 128), F32)],
        name="local",
    )(at, query, *msgs, inner, vis)
    keep, give, log_sum = call(
        join_kernel,
        [SM] + [VM] * 12,
        [((128, 256), BF16), ((128, 256), BF16), ((ROWS, 2), F32)],
        [pltpu.VMEM((ROWS, 256), BF16)],
        name="join",
    )(
        at, out, lse, rec, before, vis, gate, cumulative_gate, attention_norm_gain.reshape(1, 128),
        recurrence_norm_gain.reshape(1, 128), *got,
    )
    taken = lax.ppermute(give, "c", swap)
    shares = call(
        out_kernel,
        [SM] + [VM] * 6,
        [((32, WIDE), BF16)] * 4,
        [pltpu.VMEM((128, WIDE), BF16)],
        name="output",
    )(at, keep, taken, attention_output_weight, recurrence_output_weight, pa, pr)
    arrived = [shares[0]] + [turned(shares[o], "x", o) for o in (1, 2, 3)]
    mixed = call(add_kernel, [VM] * 4, [((32, WIDE), BF16)], name="add")(*arrived)[0]
    return (mixed, log_sum)


def solution(mesh):
    finer = Mesh(mesh.devices.reshape(4, 4, 4, 2), ("z", "y", "x", "c"))
    column = P(None, TP)
    placed = (
        P(SP, None), P(), column, column, column, P(), P(), P(SP, TP), P(TP), column, column,
        column, column, P(TP), P(SP, TP), P(TP), P(TP, None), P(TP, None),
    )
    return jax.shard_map(
        body, mesh=finer, in_specs=placed, out_specs=(P(SP + TP, None), P(SP, TP)), check_vma=False
    )
```

```python
import jax
import jax.numpy as jnp
from jax import lax
from jax.experimental import pallas as pl
from jax.experimental.pallas import tpu as pltpu
from jax.sharding import Mesh
from jax.sharding import PartitionSpec as P

HEAD_DIM = 64
EPSILON = 1e-06
ROWS = 256
WIDE = 2048
F32 = jnp.float32
BF16 = jnp.bfloat16
NEG = -1e30
SP = ("z", "y")
TP = ("x", "c")
MISC = 16
K_AT, V_AT, S_AT, M_AT, Y_ROWS = 0, 256, 512, 640, 656
O_S_AT, O_M_AT, Z_ROWS = 256, 384, 400


def dot(a, b, ca=1, cb=0):
    return lax.dot_general(a, b, (((ca,), (cb,)), ((), ())), preferred_element_type=F32)


def lanes(shape):
    return lax.broadcasted_iota(jnp.int32, shape, len(shape) - 1)


def subs(shape):
    return lax.broadcasted_iota(jnp.int32, shape, 0)


def split3(value):
    high = value.astype(BF16)
    rest = value - high.astype(F32)
    middle = rest.astype(BF16)
    low = (rest - middle.astype(F32)).astype(BF16)
    return high, middle, low


def rows_of(value):
    at_lane, at_row = lanes((MISC, 128)), subs((MISC, 128))
    out = None
    for k, part in enumerate(split3(value)):
        pick = ((at_row == k) & (at_lane == 0)) | ((at_row == 3 + k) & (at_lane == 64))
        piece = dot(jnp.where(pick, 1.0, 0.0).astype(BF16), part, 1, 1)
        out = piece if out is None else out + piece
    return out


def packed_rows(rows, extra_high, extra_low):
    first, second = rows[0:8, 0:128], rows[0:8, 128:256]
    at = subs((8, 128))
    first = jnp.where(at == 6, extra_high, jnp.where(at == 7, extra_low, first))
    return jnp.concatenate([first, second], axis=0).astype(BF16)


def spread_rows(misc):
    at_lane, at_row = lanes((MISC, 128)), subs((MISC, 128))
    halves = []
    for base in (0, 8):
        first = (at_row >= base) & (at_row < base + 3) & (at_lane < 64)
        second = (at_row >= base + 3) & (at_row < base + 6) & (at_lane >= 64)
        halves.append(dot(misc, jnp.where(first | second, 1.0, 0.0).astype(BF16), 0, 0))
    return jnp.concatenate(halves, axis=0)


def pair_of(misc):
    return misc[6:7, :].astype(F32) + misc[7:8, :].astype(F32)


def head_norm(value):
    first = lanes(value.shape) < HEAD_DIM
    squares = value * value
    one = jnp.sum(jnp.where(first, squares, 0.0), axis=-1, keepdims=True) / HEAD_DIM
    two = jnp.sum(jnp.where(first, 0.0, squares), axis=-1, keepdims=True) / HEAD_DIM
    return value * jnp.where(first, lax.rsqrt(one + EPSILON), lax.rsqrt(two + EPSILON))


def silu(value):
    return value / (1.0 + jnp.exp(-value))


def project_kernel(
    x_hbm, gain_h, wq_h, wk_h, wv_h, wrq_h, wf_h, wrv_h, wog_h, qg_h, kg_h, cum_h, slack_h, extra_h,
    again_h, rgain_h,
    q_ref, msg_ref, inner_ref, vis_ref, og_ref, cum_out, again_out, rgain_out,
    x_v, wk_v, wv_v, wq_v, wf_v, wrq_v, wrv_v, wog_v,
    gain_ref, qg_ref, kg_ref, cum_ref, slack_ref, extra_ref, again_ref, rgain_ref, sems,
):
    def begin(pairs):
        for src, dst in pairs:
            move = pltpu.make_async_copy(src, dst, sems.at[len(moves)])
            move.start()
            moves.append(move)

    moves = []
    begin([(x_hbm, x_v), (gain_h, gain_ref), (wk_h, wk_v), (wv_h, wv_v)])
    begin([(wq_h, wq_v), (wf_h, wf_v), (wrq_h, wrq_v), (wrv_h, wrv_v), (wog_h, wog_v)])
    begin([(qg_h, qg_ref), (kg_h, kg_ref), (cum_h, cum_ref), (slack_h, slack_ref)])
    begin([(extra_h, extra_ref), (again_h, again_ref), (rgain_h, rgain_ref)])
    moves[0].wait()
    moves[1].wait()
    x = x_v[...].astype(F32)
    mean = jnp.sum(x * x, axis=-1, keepdims=True) / WIDE
    normed = (x * lax.rsqrt(mean + EPSILON) * gain_ref[...]).astype(BF16)

    moves[2].wait()
    moves[3].wait()
    kv = dot(normed, jnp.concatenate([wk_v[...], wv_v[...]], axis=1))
    for move in moves[9:]:
        move.wait()
    cum_out[...] = cum_ref[...]
    again_out[...] = again_ref[...]
    rgain_out[...] = rgain_ref[...]
    kgain = jnp.concatenate([kg_ref[...], kg_ref[...]], axis=1)
    qgain = jnp.concatenate([qg_ref[...], qg_ref[...]], axis=1)
    msg_ref[K_AT:V_AT, :] = (head_norm(kv[:, 0:128]) * kgain).astype(BF16)
    msg_ref[V_AT:S_AT, :] = kv[:, 128:256].astype(BF16)

    moves[4].wait()
    moves[5].wait()
    qf = dot(normed, jnp.concatenate([wq_v[...], wf_v[...]], axis=1))
    query = (head_norm(qf[:, 0:128]) * qgain).astype(BF16)
    q_ref[...] = query * jnp.asarray(HEAD_DIM**-0.5, BF16)
    share = slack_ref[...] / (1.0 + jnp.exp(qf[:, 128:256]))
    log_keep = jnp.log1p(-share)

    moves[6].wait()
    moves[7].wait()
    rr = dot(normed, jnp.concatenate([wrq_v[...], wrv_v[...]], axis=1))
    rec_query = silu(rr[:, 0:128])
    rec_value = rr[:, 128:256].astype(BF16)
    moves[8].wait()
    og_ref[...] = silu(dot(normed, wog_v[...]))

    lower = subs((ROWS, ROWS)) >= lanes((ROWS, ROWS))
    tri = jnp.where(lower, 1.0, 0.0).astype(BF16)
    own_run = None
    for part in split3(log_keep):
        piece = dot(tri, part)
        own_run = piece if own_run is None else own_run + piece
    extra = jnp.where(lower, jnp.broadcast_to(extra_ref[...], (ROWS, ROWS)), 0.0)
    head_col = jnp.broadcast_to(jnp.sum(extra, axis=-1, keepdims=True), (ROWS, ROWS))
    head_run = head_col[:, 0:128]
    head_row = None
    for part in split3(jnp.broadcast_to(extra_ref[...], (MISC, ROWS))):
        piece = dot(part, tri, 1, 1)
        head_row = piece if head_row is None else head_row + piece
    head_row = head_row[0:1, :]
    fading = jnp.exp(jnp.where(lower, head_col - head_row, NEG))
    left = (rec_query * jnp.exp(own_run)).astype(BF16)
    right = (share * jnp.exp(-own_run)).astype(BF16)
    scores = (dot(left, right, 1, 1) * fading).astype(BF16)
    inner_ref[...] = dot(scores, rec_value)
    run = own_run + head_run
    closing = run[ROWS - 1 : ROWS, :]
    vis_ref[...] = (rec_query * jnp.exp(run)).astype(BF16)
    into = (share * jnp.exp(closing - run)).astype(BF16)
    msg_ref[S_AT:M_AT, :] = dot(rec_value, into, 0, 0).astype(BF16)
    parts = [p.astype(F32) for p in split3(-cum_ref[...])]
    rows = [p[0:1, :] for p in parts] + [p[1:2, :] for p in parts]
    rows = jnp.concatenate(rows + [jnp.zeros((2, ROWS), F32)], axis=0)
    high, middle, _ = split3(closing)
    msg_ref[M_AT:Y_ROWS, :] = packed_rows(rows, high.astype(F32), middle.astype(F32))


def spread_keys(misc, head):
    at_lane, at_row = lanes((MISC, 128)), subs((MISC, 128))
    start = HEAD_DIM * (1 - head)
    halves = []
    for base in (3 * head, 8 + 3 * head):
        pick = (at_lane - start == at_row - base) & (at_row >= base) & (at_row < base + 3)
        halves.append(dot(misc, jnp.where(pick, 1.0, 0.0).astype(BF16), 0, 0))
    return jnp.concatenate(halves, axis=0).astype(BF16)


def key_sides(msgs):
    first = lanes((ROWS, 128)) < HEAD_DIM
    keys = []
    for head in (0, 1):
        mine = first if head == 0 else ~first
        keys.append(
            jnp.concatenate(
                [jnp.where(mine, m[K_AT:V_AT, :], spread_keys(m[M_AT:Y_ROWS, :], head)) for m in msgs],
                axis=0,
            )
        )
    values = jnp.concatenate([m[V_AT:S_AT, :] for m in msgs], axis=0)
    return keys, jnp.concatenate([values, jnp.ones_like(values)], axis=1)


def attend(query, keys, values, masks):
    at = lanes((ROWS, 128))
    first = at < HEAD_DIM
    one, zero = jnp.ones_like(query), jnp.zeros_like(query)
    results = []
    for head in (0, 1):
        start = HEAD_DIM * (1 - head)
        other = jnp.where((at >= start) & (at < start + 3), one, zero)
        mine = jnp.where(first if head == 0 else ~first, query, other)
        scores = dot(mine, keys[head], 1, 1)
        if masks is not None:
            scores = jnp.where(masks, scores, NEG)
        top = jnp.max(scores, axis=-1, keepdims=True)
        weights = jnp.exp(scores - top).astype(BF16)
        summed = dot(weights, values)
        totals = summed[:, 128:256]
        results.append((summed[:, 0:128] / totals, top + jnp.log(totals)))
    return (
        jnp.where(first, results[0][0], results[1][0]),
        jnp.where(first, results[0][1], results[1][1]),
    )


def places(y):
    return [lax.rem(y - o + 4, 4) for o in range(4)]


def remote_kernel(at_ref, m0, m1, m2, m3, q1, q2, q3, o1, o2, o3, keys_ref, values_ref):
    z, y = at_ref[0], at_ref[1]
    msgs = (m0, m1, m2, m3)
    where = places(y)
    decays = [pair_of(m[M_AT:Y_ROWS, :]) for m in msgs]
    state = jnp.zeros((128, 128), F32)
    for a in range(4):
        after = jnp.zeros((1, 128), F32)
        for b in range(4):
            if b != a:
                after = after + jnp.where(where[b] > where[a], decays[b], 0.0)
        state = state + msgs[a][S_AT:M_AT, :].astype(F32) * jnp.exp(after)
    state = state.astype(BF16)
    high, middle, _ = split3(decays[0] + decays[1] + decays[2] + decays[3])

    @pl.when(z < 3)
    def _():
        keys, values = key_sides(msgs)
        keys_ref[0], keys_ref[1] = keys
        values_ref[...] = values

    for o, (query, out) in enumerate(((q1, o1), (q2, o2), (q3, o3)), 1):

        @pl.when(z + o < 4)
        def _(query=query, out=out):
            result, log_total = attend(query[...], (keys_ref[0], keys_ref[1]), values_ref[...], None)
            out[0:O_S_AT, :] = result.astype(BF16)
            out[O_S_AT:O_M_AT, :] = state
            out[O_M_AT:Z_ROWS, :] = packed_rows(
                rows_of(log_total), high.astype(F32), middle.astype(F32)
            )


def local_kernel(at_ref, q_ref, m0, m1, m2, m3, inner_ref, vis_ref, o_ref, lse_ref, rec_ref, before_ref):
    y = at_ref[1]
    msgs = (m0, m1, m2, m3)
    where = places(y)
    decays = [pair_of(m[M_AT:Y_ROWS, :]) for m in msgs]
    state = jnp.zeros((128, 128), F32)
    whole = jnp.zeros((1, 128), F32)
    for a in range(1, 4):
        between = jnp.zeros((1, 128), F32)
        for b in range(1, 4):
            if b != a:
                seen = (where[b] > where[a]) & (where[b] < y)
                between = between + jnp.where(seen, decays[b], 0.0)
        piece = msgs[a][S_AT:M_AT, :].astype(F32) * jnp.exp(between)
        state = state + jnp.where(where[a] < y, piece, 0.0)
        whole = whole + jnp.where(where[a] < y, decays[a], 0.0)
    before_ref[...] = jnp.broadcast_to(jnp.exp(whole), (8, 128))
    rec_ref[...] = inner_ref[...] + dot(vis_ref[...], state.astype(BF16), 1, 1)
    shape = (ROWS, 4 * ROWS)
    at = lanes(shape)
    earlier = subs(shape) >= at
    full = jnp.where(y >= 1, 512, 256)
    full = jnp.where(y >= 2, 768, full)
    full = jnp.where(y >= 3, 1024, full)
    masks = earlier | ((at >= 256) & (at < full))
    result, log_total = attend(q_ref[...], *key_sides(msgs), masks)
    o_ref[...] = result
    lse_ref[...] = log_total


def join_kernel(
    at_ref, o_ref, lse_ref, rec_ref, before_ref, vis_ref, og_ref, again_ref, rgain_ref, r1, r2, r3,
    keep_ref, give_ref, log_ref, both_ref,
):
    z, c = at_ref[0], at_ref[2]
    got = (r1, r2, r3)
    lses = [lse_ref[...]]
    outs = [o_ref[...]]
    for o, r in enumerate(got, 1):
        lses.append(jnp.where(z >= o, spread_rows(r[O_M_AT:Z_ROWS, :]), NEG))
        outs.append(r[0:O_S_AT, :].astype(F32))
    top = jnp.maximum(jnp.maximum(lses[0], lses[1]), jnp.maximum(lses[2], lses[3]))
    total, summed = 0.0, 0.0
    for value, out in zip(lses, outs):
        weight = jnp.exp(value - top)
        total = total + weight
        summed = summed + weight * out
    log_ref[...] = top + jnp.log(total)
    both_ref[:, 0:128] = (head_norm(summed / total) * again_ref[...]).astype(BF16)

    decays = [pair_of(r[O_M_AT:Z_ROWS, :]) for r in got]
    state = r1[O_S_AT:O_M_AT, :].astype(F32)
    state = state + r2[O_S_AT:O_M_AT, :].astype(F32) * jnp.exp(decays[0])
    state = state + r3[O_S_AT:O_M_AT, :].astype(F32) * jnp.exp(decays[0] + decays[1])
    state = (state * before_ref[0:1, :]).astype(BF16)
    rec = rec_ref[...] + dot(vis_ref[...], state, 1, 1)
    mean = jnp.sum(rec * rec, axis=-1, keepdims=True) / 128
    rec = rec * lax.rsqrt(mean + EPSILON) * rgain_ref[...] * og_ref[...]
    both_ref[:, 128:256] = rec.astype(BF16)
    for k in range(4):
        keep_ref[32 * k : 32 * k + 32, :] = both_ref[pl.ds(64 * k + 32 * c, 32), :]
        give_ref[32 * k : 32 * k + 32, :] = both_ref[pl.ds(64 * k + 32 * (1 - c), 32), :]


def log_kernel(total_ref, cum_ref, log_ref):
    rows = rows_of(total_ref[...])
    log_ref[0:1, :] = rows[0:1, :] + rows[1:2, :] + rows[2:3, :] + cum_ref[0:1, :]
    log_ref[1:2, :] = rows[3:4, :] + rows[4:5, :] + rows[5:6, :] + cum_ref[1:2, :]


def out_kernel(at_ref, keep_ref, got_ref, wa, wr, pa, pr, s0, s1, s2, s3, sum_ref):
    x = at_ref[3]
    both = jnp.concatenate([keep_ref[...], got_ref[...]], axis=1)
    for k in range(4):
        cols = slice(512 * k, 512 * k + 512)
        weight = jnp.concatenate([wa[:, cols], wr[:, cols], pa[:, cols], pr[:, cols]], axis=0)
        sum_ref[:, cols] = dot(both, weight).astype(BF16)
    for o, out in enumerate((s0, s1, s2, s3)):
        out[...] = sum_ref[pl.ds(32 * lax.rem(x + o, 4), 32), :]


def add_kernel(a, b, c, d, out):
    out[...] = (
        (a[...].astype(F32) + b[...].astype(F32)) + (c[...].astype(F32) + d[...].astype(F32))
    ).astype(BF16)


VM = pl.BlockSpec(memory_space=pltpu.VMEM)
SM = pl.BlockSpec(memory_space=pltpu.SMEM)
ANY = pl.BlockSpec(memory_space=pltpu.HBM)


def call(kernel, specs, shapes, scratch=(), name=None):
    return pl.pallas_call(
        kernel,
        in_specs=specs,
        out_specs=[VM] * len(shapes),
        out_shape=[jax.ShapeDtypeStruct(s, d) for s, d in shapes],
        scratch_shapes=list(scratch),
        compiler_params=pltpu.CompilerParams(vmem_limit_bytes=32 * 1024 * 1024),
        name=name,
    )


def far(value):
    return pltpu.with_memory_space_constraint(value, pltpu.HBM)


def turned(value, axis, by):
    return lax.ppermute(value, axis, [(i, (i + by) % 4) for i in range(4)])


def moved(value, axis, by):
    return lax.ppermute(value, axis, [(i, i + by) for i in range(4) if 0 <= i + by < 4])


def body(
    layer_input_rows, input_norm_gain, query_weight, key_weight, value_weight, query_norm_gain,
    key_norm_gain, cumulative_gate, attention_norm_gain, recurrence_query_weight, forget_weight,
    recurrence_value_weight, output_gate_weight, gate_lower_slack, extra_log_decay,
    recurrence_norm_gain, attention_output_weight, recurrence_output_weight,
):
    z, y, x, c = (lax.axis_index(a) for a in ("z", "y", "x", "c"))
    at = jnp.stack([z, y, c, x]).astype(jnp.int32)
    swap = [(0, 1), (1, 0)]
    gate_rows = cumulative_gate.T
    w = pltpu.VMEM((WIDE, 128), BF16)
    tall = (ROWS, 128)
    query, msg, inner, vis, gate, gate_near, again, rgain = call(
        project_kernel,
        [ANY] * 16,
        [(tall, BF16), ((Y_ROWS, 128), BF16), (tall, F32), (tall, BF16), (tall, F32),
         ((2, ROWS), F32), ((1, 128), F32), ((1, 128), F32)],
        [pltpu.VMEM((ROWS, WIDE), BF16)] + [w] * 7
        + [pltpu.VMEM(n, F32) for n in ((1, WIDE), (1, 64), (1, 64), (2, ROWS), (1, 128), (1, ROWS), (1, 128), (1, 128))]
        + [pltpu.SemaphoreType.DMA((16,))],
        name="project",
    )(
        *[
            far(value)
            for value in (
                layer_input_rows, input_norm_gain.reshape(1, WIDE), query_weight, key_weight,
                value_weight, recurrence_query_weight, forget_weight, recurrence_value_weight,
                output_gate_weight, query_norm_gain.reshape(1, 64), key_norm_gain.reshape(1, 64),
                gate_rows, gate_lower_slack.reshape(1, 128), extra_log_decay.T,
                attention_norm_gain.reshape(1, 128), recurrence_norm_gain.reshape(1, 128),
            )
        ]
    )
    far_msg, near_msg, back_msg = (turned(msg, "y", o) for o in (2, 1, 3))
    msgs = [msg, near_msg, far_msg, back_msg]
    queries = [moved(query, "z", -o) for o in (1, 2, 3)]
    wa, wr, _ = lax.optimization_barrier((attention_output_weight, recurrence_output_weight, query))
    pa = lax.ppermute(wa, "c", swap)
    pr = lax.ppermute(wr, "c", swap)
    sent = call(
        remote_kernel, [SM] + [VM] * 7, [((Z_ROWS, 128), BF16)] * 3,
        [pltpu.VMEM((2, 4 * ROWS, 128), BF16), pltpu.VMEM((4 * ROWS, 256), BF16)], name="remote",
    )(at, *msgs, *queries)
    got = [moved(s, "z", o) for o, s in enumerate(sent, 1)]
    out, lse, rec, before = call(
        local_kernel,
        [SM] + [VM] * 7,
        [(tall, F32), (tall, F32), (tall, F32), ((8, 128), F32)],
        name="local",
    )(at, query, *msgs, inner, vis)
    keep, give, log_total = call(
        join_kernel,
        [SM] + [VM] * 11,
        [((128, 256), BF16), ((128, 256), BF16), (tall, F32)],
        [pltpu.VMEM((ROWS, 256), BF16)],
        name="join",
    )(
        at, out, lse, rec, before, vis, gate, again, rgain, *got,
    )
    log_sum = call(log_kernel, [VM] * 2, [((2, ROWS), F32)], name="log")(log_total, gate_near)[0]
    taken = lax.ppermute(give, "c", swap)
    shares = call(
        out_kernel,
        [SM] + [VM] * 6,
        [((32, WIDE), BF16)] * 4,
        [pltpu.VMEM((128, WIDE), BF16)],
        name="output",
    )(at, keep, taken, attention_output_weight, recurrence_output_weight, pa, pr)
    arrived = [shares[0]] + [turned(shares[o], "x", o) for o in (2, 1, 3)]
    mixed = call(add_kernel, [VM] * 4, [((32, WIDE), BF16)], name="add")(*arrived)[0]
    return (mixed, log_sum.T)


def solution(mesh):
    finer = Mesh(mesh.devices.reshape(4, 4, 4, 2), ("z", "y", "x", "c"))
    column = P(None, TP)
    placed = (
        P(SP, None), P(), column, column, column, P(), P(), P(SP, TP), P(TP), column, column,
        column, column, P(TP), P(SP, TP), P(TP), P(TP, None), P(TP, None),
    )
    return jax.shard_map(
        body, mesh=finer, in_specs=placed, out_specs=(P(SP + TP, None), P(SP, TP)), check_vma=False
    )
```

```python
import jax
import jax.numpy as jnp
from jax import lax
from jax.experimental import pallas as pl
from jax.experimental.pallas import tpu as pltpu
from jax.sharding import Mesh
from jax.sharding import PartitionSpec as P


HEAD_DIM = 64
EPSILON = 1e-06
ROWS = 256
WIDE = 2048
F32 = jnp.float32
BF16 = jnp.bfloat16
NEG = -1e30
SP = ("z", "y")
TP = ("x", "c")
MISC = 16
K_AT, V_AT, S_AT, M_AT, Y_ROWS = 0, 256, 512, 640, 656
O_S_AT, O_M_AT, Z_ROWS = 256, 384, 400


def dot(a, b, ca=1, cb=0):
    return lax.dot_general(a, b, (((ca,), (cb,)), ((), ())), preferred_element_type=F32)


def lanes(shape):
    return lax.broadcasted_iota(jnp.int32, shape, len(shape) - 1)


def subs(shape):
    return lax.broadcasted_iota(jnp.int32, shape, 0)


def split3(value):
    high = value.astype(BF16)
    rest = value - high.astype(F32)
    middle = rest.astype(BF16)
    low = (rest - middle.astype(F32)).astype(BF16)
    return high, middle, low


def rows_of(value):
    at_lane, at_row = lanes((MISC, 128)), subs((MISC, 128))
    out = None
    for k, part in enumerate(split3(value)):
        pick = ((at_row == k) & (at_lane == 0)) | ((at_row == 3 + k) & (at_lane == 64))
        piece = dot(jnp.where(pick, 1.0, 0.0).astype(BF16), part, 1, 1)
        out = piece if out is None else out + piece
    return out


def packed_rows(rows, extra_high, extra_low):
    first, second = rows[0:8, 0:128], rows[0:8, 128:256]
    at = subs((8, 128))
    first = jnp.where(at == 6, extra_high, jnp.where(at == 7, extra_low, first))
    return jnp.concatenate([first, second], axis=0).astype(BF16)


def spread_rows(misc):
    at_lane, at_row = lanes((MISC, 128)), subs((MISC, 128))
    halves = []
    for base in (0, 8):
        first = (at_row >= base) & (at_row < base + 3) & (at_lane < 64)
        second = (at_row >= base + 3) & (at_row < base + 6) & (at_lane >= 64)
        halves.append(dot(misc, jnp.where(first | second, 1.0, 0.0).astype(BF16), 0, 0))
    return jnp.concatenate(halves, axis=0)


def pair_of(misc):
    return misc[6:7, :].astype(F32) + misc[7:8, :].astype(F32)


def head_norm(value):
    first = lanes(value.shape) < HEAD_DIM
    squares = value * value
    one = jnp.sum(jnp.where(first, squares, 0.0), axis=-1, keepdims=True) / HEAD_DIM
    two = jnp.sum(jnp.where(first, 0.0, squares), axis=-1, keepdims=True) / HEAD_DIM
    return value * jnp.where(first, lax.rsqrt(one + EPSILON), lax.rsqrt(two + EPSILON))


def silu(value):
    return value / (1.0 + jnp.exp(-value))


def project_kernel(
    x_hbm, gain_h, wq_h, wk_h, wv_h, wrq_h, wf_h, wrv_h, wog_h, qg_h, kg_h, cum_h, slack_h, extra_h,
    again_h, rgain_h,
    q_ref, msg_ref, inner_ref, vis_ref, og_ref, cum_out, again_out, rgain_out,
    x_v, wk_v, wv_v, wq_v, wf_v, wrq_v, wrv_v, wog_v,
    gain_ref, qg_ref, kg_ref, cum_ref, slack_ref, extra_ref, again_ref, rgain_ref, sems,
):
    def begin(pairs):
        for src, dst in pairs:
            move = pltpu.make_async_copy(src, dst, sems.at[len(moves)])
            move.start()
            moves.append(move)

    moves = []
    begin([(x_hbm, x_v), (gain_h, gain_ref), (wk_h, wk_v), (wv_h, wv_v)])
    begin([(wq_h, wq_v), (wf_h, wf_v), (wrq_h, wrq_v), (wrv_h, wrv_v), (wog_h, wog_v)])
    begin([(qg_h, qg_ref), (kg_h, kg_ref), (cum_h, cum_ref), (slack_h, slack_ref)])
    begin([(extra_h, extra_ref), (again_h, again_ref), (rgain_h, rgain_ref)])
    moves[0].wait()
    moves[1].wait()
    x = x_v[...].astype(F32)
    mean = jnp.sum(x * x, axis=-1, keepdims=True) / WIDE
    normed = (x * lax.rsqrt(mean + EPSILON) * gain_ref[...]).astype(BF16)

    moves[2].wait()
    moves[3].wait()
    kv = dot(normed, jnp.concatenate([wk_v[...], wv_v[...]], axis=1))
    for move in moves[9:]:
        move.wait()
    cum_out[...] = cum_ref[...]
    again_out[...] = again_ref[...]
    rgain_out[...] = rgain_ref[...]
    kgain = jnp.concatenate([kg_ref[...], kg_ref[...]], axis=1)
    qgain = jnp.concatenate([qg_ref[...], qg_ref[...]], axis=1)
    msg_ref[K_AT:V_AT, :] = (head_norm(kv[:, 0:128]) * kgain).astype(BF16)
    msg_ref[V_AT:S_AT, :] = kv[:, 128:256].astype(BF16)

    moves[4].wait()
    moves[5].wait()
    qf = dot(normed, jnp.concatenate([wq_v[...], wf_v[...]], axis=1))
    query = (head_norm(qf[:, 0:128]) * qgain).astype(BF16)
    q_ref[...] = query * jnp.asarray(HEAD_DIM**-0.5, BF16)
    share = slack_ref[...] / (1.0 + jnp.exp(qf[:, 128:256]))
    log_keep = jnp.log1p(-share)

    moves[6].wait()
    moves[7].wait()
    rr = dot(normed, jnp.concatenate([wrq_v[...], wrv_v[...]], axis=1))
    rec_query = silu(rr[:, 0:128])
    rec_value = rr[:, 128:256].astype(BF16)
    moves[8].wait()
    og_ref[...] = silu(dot(normed, wog_v[...]))

    lower = subs((ROWS, ROWS)) >= lanes((ROWS, ROWS))
    tri = jnp.where(lower, 1.0, 0.0).astype(BF16)
    own_run = None
    for part in split3(log_keep):
        piece = dot(tri, part)
        own_run = piece if own_run is None else own_run + piece
    extra = jnp.where(lower, jnp.broadcast_to(extra_ref[...], (ROWS, ROWS)), 0.0)
    head_col = jnp.broadcast_to(jnp.sum(extra, axis=-1, keepdims=True), (ROWS, ROWS))
    head_run = head_col[:, 0:128]
    head_row = None
    for part in split3(jnp.broadcast_to(extra_ref[...], (MISC, ROWS))):
        piece = dot(part, tri, 1, 1)
        head_row = piece if head_row is None else head_row + piece
    head_row = head_row[0:1, :]
    fading = jnp.exp(jnp.where(lower, head_col - head_row, NEG))
    left = (rec_query * jnp.exp(own_run)).astype(BF16)
    right = (share * jnp.exp(-own_run)).astype(BF16)
    scores = (dot(left, right, 1, 1) * fading).astype(BF16)
    inner_ref[...] = dot(scores, rec_value)
    run = own_run + head_run
    closing = run[ROWS - 1 : ROWS, :]
    vis_ref[...] = (rec_query * jnp.exp(run)).astype(BF16)
    into = (share * jnp.exp(closing - run)).astype(BF16)
    msg_ref[S_AT:M_AT, :] = dot(rec_value, into, 0, 0).astype(BF16)
    parts = [p.astype(F32) for p in split3(-cum_ref[...])]
    rows = [p[0:1, :] for p in parts] + [p[1:2, :] for p in parts]
    rows = jnp.concatenate(rows + [jnp.zeros((2, ROWS), F32)], axis=0)
    high, middle, _ = split3(closing)
    msg_ref[M_AT:Y_ROWS, :] = packed_rows(rows, high.astype(F32), middle.astype(F32))


def spread_keys(misc, head):
    at_lane, at_row = lanes((MISC, 128)), subs((MISC, 128))
    start = HEAD_DIM * (1 - head)
    halves = []
    for base in (3 * head, 8 + 3 * head):
        pick = (at_lane - start == at_row - base) & (at_row >= base) & (at_row < base + 3)
        halves.append(dot(misc, jnp.where(pick, 1.0, 0.0).astype(BF16), 0, 0))
    return jnp.concatenate(halves, axis=0).astype(BF16)


def key_sides(msgs):
    first = lanes((ROWS, 128)) < HEAD_DIM
    keys = []
    for head in (0, 1):
        mine = first if head == 0 else ~first
        keys.append(
            jnp.concatenate(
                [jnp.where(mine, m[K_AT:V_AT, :], spread_keys(m[M_AT:Y_ROWS, :], head)) for m in msgs],
                axis=0,
            )
        )
    values = jnp.concatenate([m[V_AT:S_AT, :] for m in msgs], axis=0)
    return keys, jnp.concatenate([values, jnp.ones_like(values)], axis=1)


def attend(query, keys, values, masks):
    at = lanes((128, 128))
    first = at < HEAD_DIM
    one, zero = jnp.ones((128, 128), BF16), jnp.zeros((128, 128), BF16)
    chains = [(row, head) for row in range(0, ROWS, 128) for head in (0, 1)]
    scores, results = {}, {}

    def score(row, head):
        start = HEAD_DIM * (1 - head)
        other = jnp.where((at >= start) & (at < start + 3), one, zero)
        mine = jnp.where(first if head == 0 else ~first, query[row : row + 128, :], other)
        found = dot(mine, keys[head], 1, 1)
        if masks is not None:
            found = jnp.where(masks[row : row + 128, :], found, NEG)
        return found

    def finish(found):
        top = jnp.max(found, axis=-1, keepdims=True)
        summed = dot(jnp.exp(found - top).astype(BF16), values)
        totals = summed[:, 128:256]
        return summed[:, 0:128] / totals, top + jnp.log(totals)

    for chain in chains:
        scores[chain] = score(*chain)
    for chain in chains:
        results[chain] = finish(scores[chain])
    return tuple(
        jnp.concatenate(
            [
                jnp.where(first, results[row, 0][k], results[row, 1][k])
                for row in range(0, ROWS, 128)
            ],
            axis=0,
        )
        for k in (0, 1)
    )


def places(y):
    return [lax.rem(y - o + 4, 4) for o in range(4)]


def remote_kernel(at_ref, m0, m1, m2, m3, q1, q2, q3, o1, o2, o3, keys_ref, values_ref):
    z, y = at_ref[0], at_ref[1]
    msgs = (m0, m1, m2, m3)
    where = places(y)
    decays = [pair_of(m[M_AT:Y_ROWS, :]) for m in msgs]
    state = jnp.zeros((128, 128), F32)
    for a in range(4):
        after = jnp.zeros((1, 128), F32)
        for b in range(4):
            if b != a:
                after = after + jnp.where(where[b] > where[a], decays[b], 0.0)
        state = state + msgs[a][S_AT:M_AT, :].astype(F32) * jnp.exp(after)
    state = state.astype(BF16)
    high, middle, _ = split3(decays[0] + decays[1] + decays[2] + decays[3])

    @pl.when(z < 3)
    def _():
        keys, values = key_sides(msgs)
        keys_ref[0], keys_ref[1] = keys
        values_ref[...] = values

    for o, (query, out) in enumerate(((q1, o1), (q2, o2), (q3, o3)), 1):

        @pl.when(z + o < 4)
        def _(query=query, out=out):
            result, log_total = attend(query[...], (keys_ref[0], keys_ref[1]), values_ref[...], None)
            out[0:O_S_AT, :] = result.astype(BF16)
            out[O_S_AT:O_M_AT, :] = state
            out[O_M_AT:Z_ROWS, :] = packed_rows(
                rows_of(log_total), high.astype(F32), middle.astype(F32)
            )


def local_kernel(at_ref, q_ref, m0, m1, m2, m3, inner_ref, vis_ref, o_ref, lse_ref, rec_ref, before_ref):
    y = at_ref[1]
    msgs = (m0, m1, m2, m3)
    where = places(y)
    decays = [pair_of(m[M_AT:Y_ROWS, :]) for m in msgs]
    state = jnp.zeros((128, 128), F32)
    whole = jnp.zeros((1, 128), F32)
    for a in range(1, 4):
        between = jnp.zeros((1, 128), F32)
        for b in range(1, 4):
            if b != a:
                seen = (where[b] > where[a]) & (where[b] < y)
                between = between + jnp.where(seen, decays[b], 0.0)
        piece = msgs[a][S_AT:M_AT, :].astype(F32) * jnp.exp(between)
        state = state + jnp.where(where[a] < y, piece, 0.0)
        whole = whole + jnp.where(where[a] < y, decays[a], 0.0)
    before_ref[...] = jnp.broadcast_to(jnp.exp(whole), (8, 128))
    rec_ref[...] = inner_ref[...] + dot(vis_ref[...], state.astype(BF16), 1, 1)
    shape = (ROWS, 4 * ROWS)
    at = lanes(shape)
    earlier = subs(shape) >= at
    full = jnp.where(y >= 1, 512, 256)
    full = jnp.where(y >= 2, 768, full)
    full = jnp.where(y >= 3, 1024, full)
    masks = earlier | ((at >= 256) & (at < full))
    result, log_total = attend(q_ref[...], *key_sides(msgs), masks)
    o_ref[...] = result
    lse_ref[...] = log_total


def join_kernel(
    at_ref, o_ref, lse_ref, rec_ref, before_ref, vis_ref, og_ref, again_ref, rgain_ref, r1, r2, r3,
    keep_ref, give_ref, log_ref, both_ref,
):
    z, c = at_ref[0], at_ref[2]
    got = (r1, r2, r3)
    lses = [lse_ref[...]]
    outs = [o_ref[...]]
    for o, r in enumerate(got, 1):
        lses.append(jnp.where(z >= o, spread_rows(r[O_M_AT:Z_ROWS, :]), NEG))
        outs.append(r[0:O_S_AT, :].astype(F32))
    top = jnp.maximum(jnp.maximum(lses[0], lses[1]), jnp.maximum(lses[2], lses[3]))
    total, summed = 0.0, 0.0
    for value, out in zip(lses, outs):
        weight = jnp.exp(value - top)
        total = total + weight
        summed = summed + weight * out
    log_ref[...] = top + jnp.log(total)
    both_ref[:, 0:128] = (head_norm(summed / total) * again_ref[...]).astype(BF16)

    decays = [pair_of(r[O_M_AT:Z_ROWS, :]) for r in got]
    state = r1[O_S_AT:O_M_AT, :].astype(F32)
    state = state + r2[O_S_AT:O_M_AT, :].astype(F32) * jnp.exp(decays[0])
    state = state + r3[O_S_AT:O_M_AT, :].astype(F32) * jnp.exp(decays[0] + decays[1])
    state = (state * before_ref[0:1, :]).astype(BF16)
    rec = rec_ref[...] + dot(vis_ref[...], state, 1, 1)
    mean = jnp.sum(rec * rec, axis=-1, keepdims=True) / 128
    rec = rec * lax.rsqrt(mean + EPSILON) * rgain_ref[...] * og_ref[...]
    both_ref[:, 128:256] = rec.astype(BF16)
    for k in range(4):
        keep_ref[32 * k : 32 * k + 32, :] = both_ref[pl.ds(64 * k + 32 * c, 32), :]
        give_ref[32 * k : 32 * k + 32, :] = both_ref[pl.ds(64 * k + 32 * (1 - c), 32), :]


def log_kernel(total_ref, cum_ref, log_ref):
    rows = rows_of(total_ref[...])
    log_ref[0:1, :] = rows[0:1, :] + rows[1:2, :] + rows[2:3, :] + cum_ref[0:1, :]
    log_ref[1:2, :] = rows[3:4, :] + rows[4:5, :] + rows[5:6, :] + cum_ref[1:2, :]


def out_kernel(at_ref, keep_ref, got_ref, wa, wr, pa, pr, s0, s1, s2, s3, sum_ref):
    x = at_ref[3]
    both = jnp.concatenate([keep_ref[...], got_ref[...]], axis=1)
    for k in range(4):
        cols = slice(512 * k, 512 * k + 512)
        weight = jnp.concatenate([wa[:, cols], wr[:, cols], pa[:, cols], pr[:, cols]], axis=0)
        sum_ref[:, cols] = dot(both, weight).astype(BF16)
    for o, out in enumerate((s0, s1, s2, s3)):
        out[...] = sum_ref[pl.ds(32 * lax.rem(x + o, 4), 32), :]


def add_kernel(a, b, c, d, out):
    out[...] = (
        (a[...].astype(F32) + b[...].astype(F32)) + (c[...].astype(F32) + d[...].astype(F32))
    ).astype(BF16)


VM = pl.BlockSpec(memory_space=pltpu.VMEM)
SM = pl.BlockSpec(memory_space=pltpu.SMEM)
ANY = pl.BlockSpec(memory_space=pltpu.HBM)


def call(kernel, specs, shapes, scratch=()):
    return pl.pallas_call(
        kernel,
        in_specs=specs,
        out_specs=[VM] * len(shapes),
        out_shape=[jax.ShapeDtypeStruct(s, d) for s, d in shapes],
        scratch_shapes=list(scratch),
        compiler_params=pltpu.CompilerParams(vmem_limit_bytes=32 * 1024 * 1024),
    )


def far(value):
    return pltpu.with_memory_space_constraint(value, pltpu.HBM)


def turned(value, axis, by):
    return lax.ppermute(value, axis, [(i, (i + by) % 4) for i in range(4)])


def moved(value, axis, by):
    return lax.ppermute(value, axis, [(i, i + by) for i in range(4) if 0 <= i + by < 4])


def body(
    layer_input_rows, input_norm_gain, query_weight, key_weight, value_weight, query_norm_gain,
    key_norm_gain, cumulative_gate, attention_norm_gain, recurrence_query_weight, forget_weight,
    recurrence_value_weight, output_gate_weight, gate_lower_slack, extra_log_decay,
    recurrence_norm_gain, attention_output_weight, recurrence_output_weight,
):
    z, y, x, c = (lax.axis_index(a) for a in ("z", "y", "x", "c"))
    at = jnp.stack([z, y, c, x]).astype(jnp.int32)
    swap = [(0, 1), (1, 0)]
    gate_rows = cumulative_gate.T
    w = pltpu.VMEM((WIDE, 128), BF16)
    tall = (ROWS, 128)
    query, msg, inner, vis, gate, gate_near, again, rgain = call(
        project_kernel,
        [ANY] * 16,
        [(tall, BF16), ((Y_ROWS, 128), BF16), (tall, F32), (tall, BF16), (tall, F32),
         ((2, ROWS), F32), ((1, 128), F32), ((1, 128), F32)],
        [pltpu.VMEM((ROWS, WIDE), BF16)] + [w] * 7
        + [pltpu.VMEM(n, F32) for n in ((1, WIDE), (1, 64), (1, 64), (2, ROWS), (1, 128), (1, ROWS), (1, 128), (1, 128))]
        + [pltpu.SemaphoreType.DMA((16,))],
    )(
        *[
            far(value)
            for value in (
                layer_input_rows, input_norm_gain.reshape(1, WIDE), query_weight, key_weight,
                value_weight, recurrence_query_weight, forget_weight, recurrence_value_weight,
                output_gate_weight, query_norm_gain.reshape(1, 64), key_norm_gain.reshape(1, 64),
                gate_rows, gate_lower_slack.reshape(1, 128), extra_log_decay.T,
                attention_norm_gain.reshape(1, 128), recurrence_norm_gain.reshape(1, 128),
            )
        ]
    )
    msgs = [msg] + [turned(msg, "y", o) for o in (1, 2, 3)]
    queries = [moved(query, "z", -o) for o in (1, 2, 3)]
    wa, wr, _ = lax.optimization_barrier((attention_output_weight, recurrence_output_weight, query))
    pa = lax.ppermute(wa, "c", swap)
    pr = lax.ppermute(wr, "c", swap)
    sent = call(
        remote_kernel, [SM] + [VM] * 7, [((Z_ROWS, 128), BF16)] * 3,
        [pltpu.VMEM((2, 4 * ROWS, 128), BF16), pltpu.VMEM((4 * ROWS, 256), BF16)],
    )(at, *msgs, *queries)
    got = [moved(s, "z", o) for o, s in enumerate(sent, 1)]
    out, lse, rec, before = call(
        local_kernel, [SM] + [VM] * 7, [(tall, F32), (tall, F32), (tall, F32), ((8, 128), F32)]
    )(at, query, *msgs, inner, vis)
    keep, give, log_total = call(
        join_kernel,
        [SM] + [VM] * 11,
        [((128, 256), BF16), ((128, 256), BF16), (tall, F32)],
        [pltpu.VMEM((ROWS, 256), BF16)],
    )(
        at, out, lse, rec, before, vis, gate, again, rgain, *got,
    )
    log_sum = call(log_kernel, [VM] * 2, [((2, ROWS), F32)])(log_total, gate_near)[0]
    taken = lax.ppermute(give, "c", swap)
    shares = call(
        out_kernel, [SM] + [VM] * 6, [((32, WIDE), BF16)] * 4, [pltpu.VMEM((128, WIDE), BF16)]
    )(at, keep, taken, attention_output_weight, recurrence_output_weight, pa, pr)
    arrived = [shares[0]] + [turned(shares[o], "x", o) for o in (1, 2, 3)]
    mixed = call(add_kernel, [VM] * 4, [((32, WIDE), BF16)])(*arrived)[0]
    return (mixed, log_sum.T)


def solution(mesh):
    finer = Mesh(mesh.devices.reshape(4, 4, 4, 2), ("z", "y", "x", "c"))
    column = P(None, TP)
    placed = (
        P(SP, None), P(), column, column, column, P(), P(), P(SP, TP), P(TP), column, column,
        column, column, P(TP), P(SP, TP), P(TP), P(TP, None), P(TP, None),
    )
    return jax.shard_map(
        body, mesh=finer, in_specs=placed, out_specs=(P(SP + TP, None), P(SP, TP)), check_vma=False
    )
```

```python
import jax
import jax.numpy as jnp
from jax import lax
from jax.experimental import pallas as pl
from jax.experimental.pallas import tpu as pltpu
from jax.sharding import Mesh
from jax.sharding import PartitionSpec as P


HEAD_DIM = 64
EPSILON = 1e-06
ROWS = 256
WIDE = 2048
F32 = jnp.float32
BF16 = jnp.bfloat16
NEG = -1e30
SP = ("z", "y")
TP = ("x", "c")
MISC = 16
K_AT, V_AT, S_AT, M_AT, Y_ROWS = 0, 256, 512, 640, 656
O_S_AT, O_M_AT, Z_ROWS = 256, 384, 400


def dot(a, b, ca=1, cb=0):
    return lax.dot_general(a, b, (((ca,), (cb,)), ((), ())), preferred_element_type=F32)


def lanes(shape):
    return lax.broadcasted_iota(jnp.int32, shape, len(shape) - 1)


def subs(shape):
    return lax.broadcasted_iota(jnp.int32, shape, 0)


def split3(value):
    high = value.astype(BF16)
    rest = value - high.astype(F32)
    middle = rest.astype(BF16)
    low = (rest - middle.astype(F32)).astype(BF16)
    return high, middle, low


def rows_of(value):
    at_lane, at_row = lanes((MISC, 128)), subs((MISC, 128))
    out = None
    for k, part in enumerate(split3(value)):
        pick = ((at_row == k) & (at_lane == 0)) | ((at_row == 3 + k) & (at_lane == 64))
        piece = dot(jnp.where(pick, 1.0, 0.0).astype(BF16), part, 1, 1)
        out = piece if out is None else out + piece
    return out


def packed_rows(rows, extra_high, extra_low):
    first, second = rows[0:8, 0:128], rows[0:8, 128:256]
    at = subs((8, 128))
    first = jnp.where(at == 6, extra_high, jnp.where(at == 7, extra_low, first))
    return jnp.concatenate([first, second], axis=0).astype(BF16)


def spread_rows(misc):
    at_lane, at_row = lanes((MISC, 128)), subs((MISC, 128))
    halves = []
    for base in (0, 8):
        first = (at_row >= base) & (at_row < base + 3) & (at_lane < 64)
        second = (at_row >= base + 3) & (at_row < base + 6) & (at_lane >= 64)
        halves.append(dot(misc, jnp.where(first | second, 1.0, 0.0).astype(BF16), 0, 0))
    return jnp.concatenate(halves, axis=0)


def pair_of(misc):
    return misc[6:7, :].astype(F32) + misc[7:8, :].astype(F32)


def head_norm(value):
    first = lanes(value.shape) < HEAD_DIM
    squares = value * value
    one = jnp.sum(jnp.where(first, squares, 0.0), axis=-1, keepdims=True) / HEAD_DIM
    two = jnp.sum(jnp.where(first, 0.0, squares), axis=-1, keepdims=True) / HEAD_DIM
    return value * jnp.where(first, lax.rsqrt(one + EPSILON), lax.rsqrt(two + EPSILON))


def silu(value):
    return value / (1.0 + jnp.exp(-value))


def project_kernel(
    x_hbm, gain_h, wq_h, wk_h, wv_h, wrq_h, wf_h, wrv_h, wog_h, qg_h, kg_h, cum_h, slack_h, extra_h,
    again_h, rgain_h,
    q_ref, msg_ref, inner_ref, vis_ref, og_ref, cum_out, again_out, rgain_out,
    x_v, wk_v, wv_v, wq_v, wf_v, wrq_v, wrv_v, wog_v,
    gain_ref, qg_ref, kg_ref, cum_ref, slack_ref, extra_ref, again_ref, rgain_ref, sems,
):
    def begin(pairs):
        for src, dst in pairs:
            move = pltpu.make_async_copy(src, dst, sems.at[len(moves)])
            move.start()
            moves.append(move)

    moves = []
    begin([(x_hbm, x_v), (gain_h, gain_ref), (wk_h, wk_v), (wv_h, wv_v)])
    begin([(wq_h, wq_v), (wf_h, wf_v), (wrq_h, wrq_v), (wrv_h, wrv_v), (wog_h, wog_v)])
    begin([(qg_h, qg_ref), (kg_h, kg_ref), (cum_h, cum_ref), (slack_h, slack_ref)])
    begin([(extra_h, extra_ref), (again_h, again_ref), (rgain_h, rgain_ref)])
    moves[0].wait()
    moves[1].wait()
    x = x_v[...].astype(F32)
    mean = jnp.sum(x * x, axis=-1, keepdims=True) / WIDE
    normed = (x * lax.rsqrt(mean + EPSILON) * gain_ref[...]).astype(BF16)

    moves[2].wait()
    moves[3].wait()
    kv = dot(normed, jnp.concatenate([wk_v[...], wv_v[...]], axis=1))
    for move in moves[9:]:
        move.wait()
    cum_out[...] = cum_ref[...]
    again_out[...] = again_ref[...]
    rgain_out[...] = rgain_ref[...]
    kgain = jnp.concatenate([kg_ref[...], kg_ref[...]], axis=1)
    qgain = jnp.concatenate([qg_ref[...], qg_ref[...]], axis=1)
    msg_ref[K_AT:V_AT, :] = (head_norm(kv[:, 0:128]) * kgain).astype(BF16)
    msg_ref[V_AT:S_AT, :] = kv[:, 128:256].astype(BF16)

    moves[4].wait()
    moves[5].wait()
    qf = dot(normed, jnp.concatenate([wq_v[...], wf_v[...]], axis=1))
    query = (head_norm(qf[:, 0:128]) * qgain).astype(BF16)
    q_ref[...] = query * jnp.asarray(HEAD_DIM**-0.5, BF16)
    share = slack_ref[...] / (1.0 + jnp.exp(qf[:, 128:256]))
    log_keep = jnp.log1p(-share)

    moves[6].wait()
    moves[7].wait()
    rr = dot(normed, jnp.concatenate([wrq_v[...], wrv_v[...]], axis=1))
    rec_query = silu(rr[:, 0:128])
    rec_value = rr[:, 128:256].astype(BF16)
    moves[8].wait()
    og_ref[...] = silu(dot(normed, wog_v[...]))

    lower = subs((ROWS, ROWS)) >= lanes((ROWS, ROWS))
    tri = jnp.where(lower, 1.0, 0.0).astype(BF16)
    high, middle, low = split3(log_keep)
    pair = dot(tri, jnp.concatenate([high, middle], axis=1))
    own_run = pair[:, 0:128] + pair[:, 128:256] + dot(tri, low)
    extra = jnp.where(lower, jnp.broadcast_to(extra_ref[...], (ROWS, ROWS)), 0.0)
    head_col = jnp.broadcast_to(jnp.sum(extra, axis=-1, keepdims=True), (ROWS, ROWS))
    head_run = head_col[:, 0:128]
    head_row = None
    for part in split3(jnp.broadcast_to(extra_ref[...], (MISC, ROWS))):
        piece = dot(part, tri, 1, 1)
        head_row = piece if head_row is None else head_row + piece
    head_row = head_row[0:1, :]
    fading = jnp.exp(jnp.where(lower, head_col - head_row, NEG))
    left = (rec_query * jnp.exp(own_run)).astype(BF16)
    right = (share * jnp.exp(-own_run)).astype(BF16)
    scores = (dot(left, right, 1, 1) * fading).astype(BF16)
    inner_ref[...] = dot(scores, rec_value)
    run = own_run + head_run
    closing = run[ROWS - 1 : ROWS, :]
    vis_ref[...] = (rec_query * jnp.exp(run)).astype(BF16)
    into = (share * jnp.exp(closing - run)).astype(BF16)
    msg_ref[S_AT:M_AT, :] = dot(rec_value, into, 0, 0).astype(BF16)
    parts = [p.astype(F32) for p in split3(-cum_ref[...])]
    rows = [p[0:1, :] for p in parts] + [p[1:2, :] for p in parts]
    rows = jnp.concatenate(rows + [jnp.zeros((2, ROWS), F32)], axis=0)
    high, middle, _ = split3(closing)
    msg_ref[M_AT:Y_ROWS, :] = packed_rows(rows, high.astype(F32), middle.astype(F32))


def spread_keys(misc, head):
    at_lane, at_row = lanes((MISC, 128)), subs((MISC, 128))
    start = HEAD_DIM * (1 - head)
    halves = []
    for base in (3 * head, 8 + 3 * head):
        pick = (at_lane - start == at_row - base) & (at_row >= base) & (at_row < base + 3)
        halves.append(dot(misc, jnp.where(pick, 1.0, 0.0).astype(BF16), 0, 0))
    return jnp.concatenate(halves, axis=0).astype(BF16)


def key_sides(msgs):
    first = lanes((ROWS, 128)) < HEAD_DIM
    keys = []
    for head in (0, 1):
        mine = first if head == 0 else ~first
        keys.append(
            jnp.concatenate(
                [jnp.where(mine, m[K_AT:V_AT, :], spread_keys(m[M_AT:Y_ROWS, :], head)) for m in msgs],
                axis=0,
            )
        )
    values = jnp.concatenate([m[V_AT:S_AT, :] for m in msgs], axis=0)
    return keys, jnp.concatenate([values, jnp.ones_like(values)], axis=1)


def attend(query, keys, values, masks):
    at = lanes((128, 128))
    first = at < HEAD_DIM
    one, zero = jnp.ones((128, 128), BF16), jnp.zeros((128, 128), BF16)
    chains = [(row, head) for row in range(0, ROWS, 128) for head in (0, 1)]
    scores, results = {}, {}

    def score(row, head):
        start = HEAD_DIM * (1 - head)
        other = jnp.where((at >= start) & (at < start + 3), one, zero)
        mine = jnp.where(first if head == 0 else ~first, query[row : row + 128, :], other)
        found = dot(mine, keys[head], 1, 1)
        if masks is not None:
            found = jnp.where(masks[row : row + 128, :], found, NEG)
        return found

    def finish(found):
        top = jnp.max(found, axis=-1, keepdims=True)
        summed = dot(jnp.exp(found - top).astype(BF16), values)
        totals = summed[:, 128:256]
        return summed[:, 0:128] / totals, top + jnp.log(totals)

    for chain in chains:
        scores[chain] = score(*chain)
    for chain in chains:
        results[chain] = finish(scores[chain])
    return tuple(
        jnp.concatenate(
            [
                jnp.where(first, results[row, 0][k], results[row, 1][k])
                for row in range(0, ROWS, 128)
            ],
            axis=0,
        )
        for k in (0, 1)
    )


def places(y):
    return [lax.rem(y - o + 4, 4) for o in range(4)]


def remote_kernel(at_ref, m0, m1, m2, m3, q1, q2, q3, o1, o2, o3, keys_ref, values_ref):
    z, y = at_ref[0], at_ref[1]
    msgs = (m0, m1, m2, m3)
    where = places(y)
    decays = [pair_of(m[M_AT:Y_ROWS, :]) for m in msgs]
    state = jnp.zeros((128, 128), F32)
    for a in range(4):
        after = jnp.zeros((1, 128), F32)
        for b in range(4):
            if b != a:
                after = after + jnp.where(where[b] > where[a], decays[b], 0.0)
        state = state + msgs[a][S_AT:M_AT, :].astype(F32) * jnp.exp(after)
    state = state.astype(BF16)
    high, middle, _ = split3(decays[0] + decays[1] + decays[2] + decays[3])

    @pl.when(z < 3)
    def _():
        keys, values = key_sides(msgs)
        keys_ref[0], keys_ref[1] = keys
        values_ref[...] = values

    for o, (query, out) in enumerate(((q1, o1), (q2, o2), (q3, o3)), 1):

        @pl.when(z + o < 4)
        def _(query=query, out=out):
            result, log_total = attend(query[...], (keys_ref[0], keys_ref[1]), values_ref[...], None)
            out[0:O_S_AT, :] = result.astype(BF16)
            out[O_S_AT:O_M_AT, :] = state
            out[O_M_AT:Z_ROWS, :] = packed_rows(
                rows_of(log_total), high.astype(F32), middle.astype(F32)
            )


def local_kernel(at_ref, q_ref, m0, m1, m2, m3, inner_ref, vis_ref, o_ref, lse_ref, rec_ref, before_ref):
    y = at_ref[1]
    msgs = (m0, m1, m2, m3)
    where = places(y)
    decays = [pair_of(m[M_AT:Y_ROWS, :]) for m in msgs]
    state = jnp.zeros((128, 128), F32)
    whole = jnp.zeros((1, 128), F32)
    for a in range(1, 4):
        between = jnp.zeros((1, 128), F32)
        for b in range(1, 4):
            if b != a:
                seen = (where[b] > where[a]) & (where[b] < y)
                between = between + jnp.where(seen, decays[b], 0.0)
        piece = msgs[a][S_AT:M_AT, :].astype(F32) * jnp.exp(between)
        state = state + jnp.where(where[a] < y, piece, 0.0)
        whole = whole + jnp.where(where[a] < y, decays[a], 0.0)
    before_ref[...] = jnp.broadcast_to(jnp.exp(whole), (8, 128))
    rec_ref[...] = inner_ref[...] + dot(vis_ref[...], state.astype(BF16), 1, 1)
    shape = (ROWS, 4 * ROWS)
    at = lanes(shape)
    earlier = subs(shape) >= at
    full = jnp.where(y >= 1, 512, 256)
    full = jnp.where(y >= 2, 768, full)
    full = jnp.where(y >= 3, 1024, full)
    masks = earlier | ((at >= 256) & (at < full))
    result, log_total = attend(q_ref[...], *key_sides(msgs), masks)
    o_ref[...] = result
    lse_ref[...] = log_total


def join_kernel(
    at_ref, o_ref, lse_ref, rec_ref, before_ref, vis_ref, og_ref, again_ref, rgain_ref, r1, r2, r3,
    keep_ref, give_ref, log_ref, both_ref,
):
    z, c = at_ref[0], at_ref[2]
    got = (r1, r2, r3)
    lses = [lse_ref[...]]
    outs = [o_ref[...]]
    for o, r in enumerate(got, 1):
        lses.append(jnp.where(z >= o, spread_rows(r[O_M_AT:Z_ROWS, :]), NEG))
        outs.append(r[0:O_S_AT, :].astype(F32))
    top = jnp.maximum(jnp.maximum(lses[0], lses[1]), jnp.maximum(lses[2], lses[3]))
    total, summed = 0.0, 0.0
    for value, out in zip(lses, outs):
        weight = jnp.exp(value - top)
        total = total + weight
        summed = summed + weight * out
    log_ref[...] = top + jnp.log(total)
    both_ref[:, 0:128] = (head_norm(summed / total) * again_ref[...]).astype(BF16)

    decays = [pair_of(r[O_M_AT:Z_ROWS, :]) for r in got]
    state = r1[O_S_AT:O_M_AT, :].astype(F32)
    state = state + r2[O_S_AT:O_M_AT, :].astype(F32) * jnp.exp(decays[0])
    state = state + r3[O_S_AT:O_M_AT, :].astype(F32) * jnp.exp(decays[0] + decays[1])
    state = (state * before_ref[0:1, :]).astype(BF16)
    rec = rec_ref[...] + dot(vis_ref[...], state, 1, 1)
    mean = jnp.sum(rec * rec, axis=-1, keepdims=True) / 128
    rec = rec * lax.rsqrt(mean + EPSILON) * rgain_ref[...] * og_ref[...]
    both_ref[:, 128:256] = rec.astype(BF16)
    for k in range(4):
        keep_ref[32 * k : 32 * k + 32, :] = both_ref[pl.ds(64 * k + 32 * c, 32), :]
        give_ref[32 * k : 32 * k + 32, :] = both_ref[pl.ds(64 * k + 32 * (1 - c), 32), :]


def log_kernel(total_ref, cum_ref, log_ref):
    rows = rows_of(total_ref[...])
    log_ref[0:1, :] = rows[0:1, :] + rows[1:2, :] + rows[2:3, :] + cum_ref[0:1, :]
    log_ref[1:2, :] = rows[3:4, :] + rows[4:5, :] + rows[5:6, :] + cum_ref[1:2, :]


def own_kernel(keep_ref, wa, wr, own_ref):
    keep = keep_ref[...]
    for k in range(4):
        cols = slice(512 * k, 512 * k + 512)
        own_ref[:, cols] = dot(keep, jnp.concatenate([wa[:, cols], wr[:, cols]], axis=0))


def out_kernel(at_ref, own_ref, got_ref, pa, pr, s0, s1, s2, s3, sum_ref):
    x = at_ref[3]
    got = got_ref[...]
    for k in range(4):
        cols = slice(512 * k, 512 * k + 512)
        weight = jnp.concatenate([pa[:, cols], pr[:, cols]], axis=0)
        sum_ref[:, cols] = (own_ref[:, cols] + dot(got, weight)).astype(BF16)
    for o, out in enumerate((s0, s1, s2, s3)):
        out[...] = sum_ref[pl.ds(32 * lax.rem(x + o, 4), 32), :]


def add_kernel(a, b, c, d, out):
    out[...] = (
        (a[...].astype(F32) + b[...].astype(F32)) + (c[...].astype(F32) + d[...].astype(F32))
    ).astype(BF16)


VM = pl.BlockSpec(memory_space=pltpu.VMEM)
SM = pl.BlockSpec(memory_space=pltpu.SMEM)
ANY = pl.BlockSpec(memory_space=pltpu.HBM)


def call(kernel, specs, shapes, scratch=()):
    return pl.pallas_call(
        kernel,
        in_specs=specs,
        out_specs=[VM] * len(shapes),
        out_shape=[jax.ShapeDtypeStruct(s, d) for s, d in shapes],
        scratch_shapes=list(scratch),
        compiler_params=pltpu.CompilerParams(vmem_limit_bytes=32 * 1024 * 1024),
    )


def far(value):
    return pltpu.with_memory_space_constraint(value, pltpu.HBM)


def turned(value, axis, by):
    return lax.ppermute(value, axis, [(i, (i + by) % 4) for i in range(4)])


def moved(value, axis, by):
    return lax.ppermute(value, axis, [(i, i + by) for i in range(4) if 0 <= i + by < 4])


def body(
    layer_input_rows, input_norm_gain, query_weight, key_weight, value_weight, query_norm_gain,
    key_norm_gain, cumulative_gate, attention_norm_gain, recurrence_query_weight, forget_weight,
    recurrence_value_weight, output_gate_weight, gate_lower_slack, extra_log_decay,
    recurrence_norm_gain, attention_output_weight, recurrence_output_weight,
):
    z, y, x, c = (lax.axis_index(a) for a in ("z", "y", "x", "c"))
    at = jnp.stack([z, y, c, x]).astype(jnp.int32)
    swap = [(0, 1), (1, 0)]
    gate_rows = cumulative_gate.T
    w = pltpu.VMEM((WIDE, 128), BF16)
    tall = (ROWS, 128)
    query, msg, inner, vis, gate, gate_near, again, rgain = call(
        project_kernel,
        [ANY] * 16,
        [(tall, BF16), ((Y_ROWS, 128), BF16), (tall, F32), (tall, BF16), (tall, F32),
         ((2, ROWS), F32), ((1, 128), F32), ((1, 128), F32)],
        [pltpu.VMEM((ROWS, WIDE), BF16)] + [w] * 7
        + [pltpu.VMEM(n, F32) for n in ((1, WIDE), (1, 64), (1, 64), (2, ROWS), (1, 128), (1, ROWS), (1, 128), (1, 128))]
        + [pltpu.SemaphoreType.DMA((16,))],
    )(
        *[
            far(value)
            for value in (
                layer_input_rows, input_norm_gain.reshape(1, WIDE), query_weight, key_weight,
                value_weight, recurrence_query_weight, forget_weight, recurrence_value_weight,
                output_gate_weight, query_norm_gain.reshape(1, 64), key_norm_gain.reshape(1, 64),
                gate_rows, gate_lower_slack.reshape(1, 128), extra_log_decay.T,
                attention_norm_gain.reshape(1, 128), recurrence_norm_gain.reshape(1, 128),
            )
        ]
    )
    msgs = [msg] + [turned(msg, "y", o) for o in (1, 2, 3)]
    queries = [moved(query, "z", -o) for o in (1, 2, 3)]
    wa, wr, _ = lax.optimization_barrier((attention_output_weight, recurrence_output_weight, query))
    pa = lax.ppermute(wa, "c", swap)
    pr = lax.ppermute(wr, "c", swap)
    sent = call(
        remote_kernel, [SM] + [VM] * 7, [((Z_ROWS, 128), BF16)] * 3,
        [pltpu.VMEM((2, 4 * ROWS, 128), BF16), pltpu.VMEM((4 * ROWS, 256), BF16)],
    )(at, *msgs, *queries)
    got = [moved(s, "z", o) for o, s in enumerate(sent, 1)]
    out, lse, rec, before = call(
        local_kernel, [SM] + [VM] * 7, [(tall, F32), (tall, F32), (tall, F32), ((8, 128), F32)]
    )(at, query, *msgs, inner, vis)
    keep, give, log_total = call(
        join_kernel,
        [SM] + [VM] * 11,
        [((128, 256), BF16), ((128, 256), BF16), (tall, F32)],
        [pltpu.VMEM((ROWS, 256), BF16)],
    )(
        at, out, lse, rec, before, vis, gate, again, rgain, *got,
    )
    log_sum = call(log_kernel, [VM] * 2, [((2, ROWS), F32)])(log_total, gate_near)[0]
    taken = lax.ppermute(give, "c", swap)
    own = call(own_kernel, [VM] * 3, [((128, WIDE), F32)])(
        keep, attention_output_weight, recurrence_output_weight
    )[0]
    shares = call(
        out_kernel, [SM] + [VM] * 4, [((32, WIDE), BF16)] * 4, [pltpu.VMEM((128, WIDE), BF16)]
    )(at, own, taken, pa, pr)
    arrived = [shares[0]] + [turned(shares[o], "x", o) for o in (1, 2, 3)]
    mixed = call(add_kernel, [VM] * 4, [((32, WIDE), BF16)])(*arrived)[0]
    return (mixed, log_sum.T)


def solution(mesh):
    finer = Mesh(mesh.devices.reshape(4, 4, 4, 2), ("z", "y", "x", "c"))
    column = P(None, TP)
    placed = (
        P(SP, None), P(), column, column, column, P(), P(), P(SP, TP), P(TP), column, column,
        column, column, P(TP), P(SP, TP), P(TP), P(TP, None), P(TP, None),
    )
    return jax.shard_map(
        body, mesh=finer, in_specs=placed, out_specs=(P(SP + TP, None), P(SP, TP)), check_vma=False
    )
```
